256 devices in a mesh: grp: 2 (over y), ep: 32 (over z, core), tp: 4 (over x).
Axes of the slice: x: 4, y: 2, z: 16, core: 2. Of those that a mesh axis runs over, the one named last changes fastest.
The devices are a block of a 4x16x16 slice.
Arguments:
- mixer_input: bfloat16 [32768, 2048], P(('grp', 'ep', 'tp')), parts along dimension 0, may hold values from -8 to 8
- forget_cumsum: float32 [8, 32768], P('tp', 'grp'), parts along dimension 1, may hold values from -2051 to 0, as said below
- mixer_gain: float32 [2048], replicated, may hold values from 0.1 to 1.9
- query_weight: bfloat16 [2048, 1024], P(None, 'tp'), may hold values from -6 to 6
- key_weight: bfloat16 [2048, 1024], P(None, 'tp'), may hold values from -6 to 6
- value_weight: bfloat16 [2048, 1024], P(None, 'tp'), may hold values from -0.125 to 0.125
- out_weight: bfloat16 [1024, 2048], P('tp'), may hold values from -0.1875 to 0.1875
- post_gain: float32 [2048], replicated, may hold values from 0.1 to 1.9
- expert_input: bfloat16 [32768, 2048], P(('grp', 'ep', 'tp')), parts along dimension 0, may hold values from -6 to 6
- expert_gain: float32 [2048], replicated, may hold values from 0.1 to 1.9
- routes: int32 [32768, 2], P(('grp', 'ep', 'tp')), parts along dimension 0, may hold values from 0 to 31, all different within a row; in each aligned block of 128 rows (0 to 127, 128 to 255, ...) at most 9 rows name the same one
- route_weight: float32 [32768, 2], P(('grp', 'ep', 'tp')), parts along dimension 0, may hold values from 0.2 to 1
- expert_gate: bfloat16 [32, 2048, 2048], P('ep', None, 'tp'), may hold values from -0.125 to 0.125
- expert_upward: bfloat16 [32, 2048, 2048], P('ep', None, 'tp'), may hold values from -0.125 to 0.125
- expert_down: bfloat16 [32, 2048, 2048], P('ep', 'tp'), may hold values from -0.125 to 0.125
Outputs:
- mixer_output: bfloat16 [32768, 2048], P(('grp', 'ep', 'tp')), parts along dimension 0
- expert_output: bfloat16 [32768, 2048], P(('grp', 'ep', 'tp')), parts along dimension 0
The draws below stay inside these ranges and needn't reach their ends.
There are 2 independent parts, one for each index of `grp`. The reference program is written for one: setup_inputs(seed, part) draws one part's arguments, and reference() takes and returns one part's arrays. A program takes and returns all parts, laid end to end along the dimension named above; an argument that names none is the same for every part. Nothing has to cross between parts.
Inputs may be any that keep to these rules, and one draw needn't show every extreme that they name: `forget_cumsum`: each head's row never rises along positions. `routes`: A row names 2 different experts. Within the rows of one device (aligned blocks of 128 rows) no expert is named by more than 9 rows, and in every draw some expert is named by exactly 9 rows of some block.
All inputs are finite; a program needn't handle non-finite values.
Results may differ from the reference program's by a relative error of at most 0.012.
Values may be sent and summed in bfloat16 or wider, within the bound.
A program may use at most 128 MiB of HBM per device.

```python
import math
import jax
import jax.numpy as jnp
import numpy as np
from jax import lax

D = 2048
ATTENDER_NUMBER = 8
HEAD_DIM = 128
EXP_FF = 2048
TOP = 2
MOE_ROWS = 128
SPAN = 512
WINDOW_EXTENT = 16384
TOK_MOE = 16384
EXPERTS = 32
CAP = 9
N_EP = 32
N_TP = 4


def draw_mixer_input(key, part):
    base = jnp.clip(jax.random.normal(jax.random.fold_in(key, 1), (WINDOW_EXTENT, D), jnp.float32), -6.0, 6.0)
    return base.astype(jnp.bfloat16)


def base_weight(key, number):
    normal = jax.random.normal(jax.random.fold_in(key, number), (D, ATTENDER_NUMBER * HEAD_DIM), jnp.float32)
    return jnp.clip(normal, -6.0, 6.0) * D ** (-0.5)


def draw_query_weight(key, part):
    return base_weight(key, 101).astype(jnp.bfloat16)


def draw_key_weight(key, part):
    return base_weight(key, 202).astype(jnp.bfloat16)


def draw_forget_cumsum(key, part):
    order = jax.random.permutation(jax.random.fold_in(key, 1), ATTENDER_NUMBER)
    fast_count = ATTENDER_NUMBER // 2
    rapid_route = order < fast_count
    fast_rate = jnp.exp(jax.random.uniform(jax.random.fold_in(key, 2), (ATTENDER_NUMBER,), jnp.float32, math.log(1.0 / 100.0), math.log(1.0 / 30.0)))
    slow_rate = 0.4 / WINDOW_EXTENT * jnp.exp(jax.random.uniform(jax.random.fold_in(key, 3), (ATTENDER_NUMBER,), jnp.float32, math.log(0.7), math.log(1.4)))
    rate = jnp.where(rapid_route, fast_rate, slow_rate)
    factor = jnp.exp(jax.random.uniform(jax.random.fold_in(key, 4), (ATTENDER_NUMBER, WINDOW_EXTENT // SPAN), jnp.float32, math.log(0.5), math.log(2.0)))
    factor = jnp.repeat(factor, SPAN, axis=1)
    jitter = jax.random.uniform(jax.random.fold_in(key, 5), (ATTENDER_NUMBER, WINDOW_EXTENT), jnp.float32, 0.3, 1.7)
    advance_increment = -rate[:, None] * factor * jitter
    flurry_slot = jax.random.randint(jax.random.fold_in(key, 6), (ATTENDER_NUMBER, 3), 0, WINDOW_EXTENT)
    flurry_extent = jnp.log(jax.random.uniform(jax.random.fold_in(key, 7), (ATTENDER_NUMBER, 3), jnp.float32, 0.5, 0.8))
    element_place = jnp.arange(WINDOW_EXTENT, dtype=jnp.int32)
    agreeing_tally = element_place[None, None, :] == flurry_slot[:, :, None]
    flurry_clusters = jnp.sum(jnp.where(agreeing_tally, flurry_extent[:, :, None], 0.0), axis=1)
    flurry_clusters = flurry_clusters * jnp.where(rapid_route, 0.0, 1.0)[:, None]
    return jnp.cumsum(advance_increment + flurry_clusters, axis=1)


def steps_of(key, dims, split, low, high):
    level = 1.0
    for dim, blocks in split:
        steps = jax.random.uniform(jax.random.fold_in(jax.random.fold_in(key, 6), dim), (blocks,), jnp.float32, low / len(split), high / len(split))
        level = level * jnp.repeat(jnp.exp(steps), dims[dim] // blocks).reshape((-1,) + (1,) * (len(dims) - 1 - dim))
    return level


def shared_out(key, own, number, rows, count, top, reach, skew):
    order = jax.random.permutation(key, count)
    packed, common = load_shares(count, rows * top, reach, skew, True), load_shares(count, rows * top, reach, skew, False)
    places = jnp.arange(count)

    def named(tallies, turn):
        used = int((tallies > 0).sum())
        fixed = max(1, used // 4)
        shifted = fixed + (places - fixed + turn * (used - fixed)) % max(1, count - fixed)
        return jnp.zeros((count,), jnp.int32).at[order[jnp.where(places < fixed, places, shifted)]].set(jnp.asarray(tallies, jnp.int32))

    tallies = jnp.where(number % 4 == 0, named(packed, number // 4), named(common, number - number // 4 - 1))
    mixed = jax.random.permutation(jax.random.fold_in(own, 3), count)
    donor, receiver = mixed[0:count // 2 * 2:2], mixed[1:count // 2 * 2:2]
    margin = jnp.minimum(tallies[donor] - 1, reach - tallies[receiver]) // 2
    margin = jnp.where((donor == order[0]) | (receiver == order[0]) | (tallies[receiver] == 0), 0, jnp.maximum(margin, 0))
    shifted = jax.random.randint(jax.random.fold_in(own, 4), (count // 2,), 0, 1 << 20) % (margin + 1)
    tallies = tallies.at[donor].add(-shifted).at[receiver].add(shifted)
    items = jnp.searchsorted(jnp.cumsum(tallies), jnp.arange(rows * top), side="right").astype(jnp.int32)
    listing = items.reshape(top, rows).T
    listing = listing[jax.random.permutation(jax.random.fold_in(own, 1), rows)]
    turn = jax.random.randint(jax.random.fold_in(own, 2), (rows, 1), 0, top)
    return jnp.take_along_axis(listing, (jnp.arange(top)[None, :] + turn) % top, axis=1)


def load_shares(amount, total, bound, skew, full):
    weights = [(1 << 20) // math.isqrt(standing ** skew) + 1 for standing in range(1, amount + 1)]
    largest = bound if full else min(bound, max(-(-total // amount), total * weights[0] // sum(weights)))
    least = 1 if total - largest >= amount - 1 else 0
    counts, surplus = [largest] + [least] * (amount - 1), total - largest - least * (amount - 1)
    while surplus > 0:
        movable = [i for i in range(1, amount) if counts[i] < largest] or [i for i in range(1, amount) if counts[i] < bound]
        mass, budget = sum([weights[i] for i in movable]), surplus
        for i in movable:
            addition = min(bound - counts[i], max(1, budget * weights[i] // mass), surplus)
            counts[i] = counts[i] + addition
            surplus = surplus - addition
    return np.array(counts)


def gaussian(stream_key, shape, scale, most, split=(), held_as=jnp.bfloat16):
    level = steps_of(stream_key, shape, split, -0.22, 0.18) if split else 1.0
    result = jax.random.normal(stream_key, shape, jnp.float32) * scale * level
    return jnp.minimum(jnp.maximum(result, -most), most).astype(held_as)


def setup_inputs(seed: int = 0, part: int = 0) -> dict:
    keys = jax.random.split(jax.random.key(seed), 16)
    own_keys = jax.random.split(jax.random.fold_in(keys[15], part), 16)
    mixer_input = draw_mixer_input(jax.random.fold_in(jax.random.fold_in(keys[15], part), 71), part)
    forget_cumsum = draw_forget_cumsum(jax.random.fold_in(jax.random.fold_in(keys[15], part), 71), part)
    mixer_gain = jnp.clip(1.0 + 0.18 * jax.random.normal(keys[2], (D,), jnp.float32), 0.1, 1.9)
    query_weight = draw_query_weight(jax.random.fold_in(keys[15], 71), part)
    key_weight = draw_key_weight(jax.random.fold_in(keys[15], 71), part)
    value_weight = gaussian(keys[5], (D, ATTENDER_NUMBER * HEAD_DIM), D ** -0.5, 0.125, ((1, 4),))
    out_weight = gaussian(keys[6], (ATTENDER_NUMBER * HEAD_DIM, D), (ATTENDER_NUMBER * HEAD_DIM) ** -0.5, 0.1875, ((0, 4),))
    post_gain = jnp.clip(1.0 + 0.18 * jax.random.normal(keys[7], (D,), jnp.float32), 0.1, 1.9)
    expert_input = gaussian(own_keys[8], (TOK_MOE, D), 1.0, 6.0, ((0, 128),))
    expert_gain = jnp.clip(1.0 + 0.18 * jax.random.normal(keys[9], (D,), jnp.float32), 0.1, 1.9)
    routes_keys = jax.random.split(jax.random.fold_in(own_keys[10], 1), TOK_MOE // MOE_ROWS)
    routes_turns = jax.random.permutation(jax.random.fold_in(own_keys[10], 3), TOK_MOE // MOE_ROWS)
    routes = jax.vmap(lambda own, number: shared_out(jax.random.fold_in(own_keys[10], 2), own, number, MOE_ROWS, EXPERTS, TOP, CAP, 2))(routes_keys, routes_turns).reshape((TOK_MOE, TOP))
    route_weight = jnp.clip(0.2 + 0.8 * jax.random.uniform(own_keys[11], (TOK_MOE, TOP), jnp.float32) ** steps_of(own_keys[11], (TOK_MOE, TOP), ((0, 128),), -0.2, 0.2), 0.2, 1.0)
    expert_gate = gaussian(keys[12], (EXPERTS, D, EXP_FF), D ** -0.5, 0.125, ((0, 32), (2, 4)))
    expert_upward = gaussian(keys[13], (EXPERTS, D, EXP_FF), D ** -0.5, 0.125, ((0, 32), (2, 4)))
    expert_down = gaussian(keys[14], (EXPERTS, EXP_FF, D), EXP_FF ** -0.5, 0.125, ((0, 32), (1, 4)))
    return dict(mixer_input=mixer_input, forget_cumsum=forget_cumsum, mixer_gain=mixer_gain, query_weight=query_weight, key_weight=key_weight, value_weight=value_weight, out_weight=out_weight, post_gain=post_gain, expert_input=expert_input, expert_gain=expert_gain, routes=routes, route_weight=route_weight, expert_gate=expert_gate, expert_upward=expert_upward, expert_down=expert_down)


EPS = 1e-06
MASKED = -1e+30

def normalize(rows, gain):
    values = rows.astype(jnp.float32)
    inverse = lax.rsqrt(lax.optimization_barrier(jnp.mean(values * values, axis=-1, keepdims=True)) + EPS)
    return values * inverse * gain.astype(jnp.float32)

def attend(queries, key_rows, value_rows, forget_cumsum):
    head_q = queries.reshape(WINDOW_EXTENT, ATTENDER_NUMBER, HEAD_DIM).transpose(1, 0, 2).astype(jnp.float32)
    head_k = key_rows.reshape(WINDOW_EXTENT, ATTENDER_NUMBER, HEAD_DIM).transpose(1, 0, 2).astype(jnp.float32)
    head_v = value_rows.reshape(WINDOW_EXTENT, ATTENDER_NUMBER, HEAD_DIM).transpose(1, 0, 2).astype(jnp.float32)
    block_size = math.gcd(WINDOW_EXTENT, 512)

    def one_query_block(block_index):
        first_row = block_index * block_size
        query_block = lax.dynamic_slice_in_dim(head_q, first_row, block_size, 1)
        query_gate = lax.dynamic_slice_in_dim(forget_cumsum, first_row, block_size, 1)
        query_pos = first_row + jnp.arange(block_size, dtype=jnp.int32)

        def advance_increment(key_index, state):
            running_max, running_sum, running_acc = state
            key_first = key_index * block_size
            key_block = lax.dynamic_slice_in_dim(head_k, key_first, block_size, 1)
            value_block = lax.dynamic_slice_in_dim(head_v, key_first, block_size, 1)
            key_gate = lax.dynamic_slice_in_dim(forget_cumsum, key_first, block_size, 1)
            scores = jnp.einsum('hqd,hkd->hqk', query_block, key_block) * HEAD_DIM ** (-0.5)
            scores = scores + query_gate[:, :, None] - key_gate[:, None, :]
            key_pos = key_first + jnp.arange(block_size, dtype=jnp.int32)
            visible = (key_pos[None, :] <= query_pos[:, None])[None]
            scores = jnp.where(visible, scores, MASKED)
            new_max = jnp.maximum(running_max, lax.optimization_barrier(jnp.max(scores, axis=-1)))
            weights = jnp.where(visible, jnp.exp(scores - new_max[..., None]), 0.0)
            rescale = jnp.exp(running_max - new_max)
            running_sum = running_sum * rescale + lax.optimization_barrier(jnp.sum(weights, axis=-1))
            rounded = lax.optimization_barrier(weights.astype(jnp.bfloat16)).astype(jnp.float32)
            running_acc = running_acc * rescale[..., None] + jnp.einsum('hqk,hkd->hqd', rounded, value_block)
            return (new_max, running_sum, running_acc)
        initial = (jnp.full((ATTENDER_NUMBER, block_size), MASKED, jnp.float32), jnp.zeros((ATTENDER_NUMBER, block_size), jnp.float32), jnp.zeros((ATTENDER_NUMBER, block_size, HEAD_DIM), jnp.float32))
        running_max, running_sum, running_acc = lax.fori_loop(0, block_index + 1, advance_increment, initial)
        return (running_acc / running_sum[..., None]).astype(jnp.bfloat16)
    blocks = lax.map(one_query_block, jnp.arange(WINDOW_EXTENT // block_size, dtype=jnp.int32))
    return blocks.transpose(0, 2, 1, 3).reshape(WINDOW_EXTENT, ATTENDER_NUMBER * HEAD_DIM)

def one_expert(operands):
    rows, gate_part, upward_part, down_part = operands
    group = EXP_FF // N_TP
    running = jnp.zeros((rows.shape[0], D), jnp.float32)
    for shard in range(N_TP):
        gate_proj = jnp.dot(rows, gate_part[:, shard * group:(shard + 1) * group], preferred_element_type=jnp.float32)
        upward = jnp.dot(rows, upward_part[:, shard * group:(shard + 1) * group], preferred_element_type=jnp.float32)
        hidden = (jax.nn.silu(gate_proj) * upward).astype(jnp.bfloat16)
        partial_term = jnp.dot(hidden, down_part[shard * group:(shard + 1) * group, :], preferred_element_type=jnp.float32)
        running = running + lax.optimization_barrier(partial_term.astype(jnp.bfloat16)).astype(jnp.float32)
    return running.astype(jnp.bfloat16)

def reference(mixer_input, forget_cumsum, mixer_gain, query_weight, key_weight, value_weight, out_weight, post_gain, expert_input, expert_gain, routes, route_weight, expert_gate, expert_upward, expert_down):
    normed = normalize(mixer_input, mixer_gain).astype(jnp.bfloat16)
    queries = jnp.dot(normed, query_weight, preferred_element_type=jnp.float32).astype(jnp.bfloat16)
    key_rows = jnp.dot(normed, key_weight, preferred_element_type=jnp.float32).astype(jnp.bfloat16)
    value_rows = jnp.dot(normed, value_weight, preferred_element_type=jnp.float32).astype(jnp.bfloat16)
    attended = attend(queries, key_rows, value_rows, forget_cumsum)
    group = ATTENDER_NUMBER * HEAD_DIM // N_TP
    mixer_sum = jnp.zeros((WINDOW_EXTENT, D), jnp.float32)
    for shard in range(N_TP):
        partial_term = jnp.dot(attended[:, shard * group:(shard + 1) * group], out_weight[shard * group:(shard + 1) * group, :], preferred_element_type=jnp.float32)
        mixer_sum = mixer_sum + lax.optimization_barrier(partial_term.astype(jnp.bfloat16)).astype(jnp.float32)
    mixer_output = normalize(mixer_sum, post_gain).astype(jnp.bfloat16)
    sources = N_EP * N_TP
    normed_moe = normalize(expert_input, expert_gain).astype(jnp.bfloat16)
    grouped = routes.reshape(sources, MOE_ROWS * TOP).astype(jnp.int32)
    member = (grouped[:, :, None] == jnp.arange(EXPERTS, dtype=jnp.int32)[None, None, :]).astype(jnp.int32)
    before = jnp.cumsum(member, axis=1) - member
    slot_rank = lax.optimization_barrier(jnp.sum(before * member, axis=-1))
    slot_index = grouped * (sources * CAP) + jnp.arange(sources, dtype=jnp.int32)[:, None] * CAP + slot_rank
    slot_index = slot_index.reshape(-1).astype(jnp.int32)
    repeated = jnp.repeat(normed_moe, TOP, axis=0)
    buffer = jnp.zeros((EXPERTS * sources * CAP, D), jnp.bfloat16).at[slot_index].set(repeated)
    buffer = buffer.reshape(EXPERTS, sources * CAP, D)
    outputs = lax.map(one_expert, (buffer, expert_gate, expert_upward, expert_down)).reshape(-1, D)
    picked = outputs[slot_index].reshape(TOK_MOE, TOP, D).astype(jnp.float32)
    expert_output = lax.optimization_barrier(jnp.sum(picked * route_weight.astype(jnp.float32)[:, :, None], axis=1)).astype(jnp.bfloat16)
    return (mixer_output, expert_output)
```

```python
import functools

import jax
import jax.numpy as jnp
from jax import lax
from jax.experimental import pallas as pl
from jax.experimental.pallas import tpu as pltpu
from jax.sharding import PartitionSpec as P

EPS = 1e-06
MASKED = -1e30
LOG2E = 1.4426950408889634
MESH = pl.DeviceIdType.MESH
SUB, LANE = 16, 128
BF16, F32 = jnp.bfloat16, jnp.float32
ANY = pl.BlockSpec(memory_space=pl.ANY)
VM = pl.BlockSpec(memory_space=pltpu.VMEM)


def normalize(row_block, gain):
    values = row_block.astype(F32)
    inverse = lax.rsqrt(jnp.mean(values * values, axis=-1, keepdims=True) + EPS)
    return values * inverse * gain


def dot(a, b):
    return jnp.dot(a, b, preferred_element_type=F32)


def swap_matrix():
    n = SUB * SUB
    i = lax.broadcasted_iota(jnp.int32, (n, n), 0)
    k = lax.broadcasted_iota(jnp.int32, (n, n), 1)
    hit = ((i // SUB) == (k % SUB)) & ((i % SUB) == (k // SUB))
    return jnp.where(hit, 1.0, 0.0).astype(BF16)


def to_wire(swap, rows):
    halves = [
        jnp.concatenate(
            [rows[SUB * a : SUB * (a + 1), LANE * s : LANE * (s + 1)] for s in range(SUB)], axis=0
        )
        for a in range(2)
    ]
    out = dot(swap, jnp.concatenate(halves, axis=1)).astype(BF16)
    return jnp.concatenate([out[:, :LANE], out[:, LANE:]], axis=0)


def from_wire(swap, tiles):
    n = SUB * SUB
    out = dot(swap, jnp.concatenate([tiles[:n], tiles[n:]], axis=1)).astype(BF16)
    halves = [
        jnp.concatenate(
            [out[SUB * s : SUB * (s + 1), LANE * a : LANE * (a + 1)] for s in range(SUB)], axis=1
        )
        for a in range(2)
    ]
    return jnp.concatenate(halves, axis=0)


def slot_columns(routes, capacity):
    rows, top = routes.shape
    experts = lax.broadcasted_iota(jnp.int32, (rows, LANE), 1)
    earlier = lax.broadcasted_iota(jnp.int32, (rows, rows), 1) < lax.broadcasted_iota(
        jnp.int32, (rows, rows), 0
    )
    earlier = jnp.where(earlier, 1.0, 0.0).astype(BF16)
    taken = jnp.zeros((1, LANE), F32)
    columns = []
    for k in range(top):
        member = jnp.where(experts == routes[:, k : k + 1], 1.0, 0.0)
        before = dot(earlier, member.astype(BF16)) + taken
        rank = jnp.sum(before * member, axis=1, keepdims=True)
        columns.append(routes[:, k : k + 1].astype(F32) * capacity + rank)
        taken = taken + jnp.sum(member, axis=0, keepdims=True)
    return columns


def chooser(column, width):
    ids = lax.broadcasted_iota(jnp.int32, (column.shape[0], width), 1).astype(F32)
    return jnp.where(ids == column, 1.0, 0.0)


def greet(axes):
    barrier = pltpu.get_barrier_semaphore()
    total = 0
    for axis in axes:
        n = lax.axis_size(axis)
        me = lax.axis_index(axis)

        @pl.loop(1, n)
        def _(s):
            pl.semaphore_signal(
                barrier, inc=1, device_id={axis: lax.rem(me + s, n)}, device_id_type=MESH
            )

        total += n - 1
    return lambda: pl.semaphore_wait(barrier, total)


def exchange(send, land, block, send_sem, recv_sem):
    n = lax.axis_size("ep")
    me = lax.axis_index("ep")

    def copy(s):
        to = lax.rem(me + s, n)
        return pltpu.make_async_remote_copy(
            src_ref=send.at[pl.ds(pl.multiple_of(to * block, block), block)],
            dst_ref=land.at[pl.ds(pl.multiple_of(me * block, block), block)],
            send_sem=send_sem.at[s],
            recv_sem=recv_sem.at[s],
            device_id={"ep": to},
            device_id_type=MESH,
        )

    def start():
        half = n // 2

        @pl.loop(1, half)
        def _(s):
            copy(s).start()
            copy(n - s).start()

        copy(half).start()

    def wait():
        @pl.loop(1, n)
        def _(s):
            copy(s).wait()

    return start, wait


def first_kernel(
    capacity,
    x_ref, gain_ref, wq_ref, wk_ref, wv_ref, y_ref, ygain_ref, routes_ref,
    q_ref, kv_ref, land_ref,
    normed, weights, picked, send, w_sem, xs_sem, xr_sem, zs_sem, zr_sem,
):
    rows, width = x_ref.shape
    head_width = wq_ref.shape[1]
    tp, t = lax.axis_size("tp"), lax.axis_index("tp")
    ep, e = lax.axis_size("ep"), lax.axis_index("ep")
    slots = picked.shape[0]
    block = capacity * SUB
    loads = [
        pltpu.make_async_copy(w, weights.at[i], w_sem.at[i])
        for i, w in enumerate((wq_ref, wk_ref, wv_ref))
    ]
    for load in loads:
        load.start()
    met = greet(("ep", "tp"))

    own = pl.ds(pl.multiple_of(t * rows, rows), rows)
    normed[own, :] = normalize(x_ref[...], gain_ref[...]).astype(BF16)
    columns = slot_columns(routes_ref[...], capacity)
    padded = -(-slots // LANE) * LANE
    choose = sum(chooser(c, padded) for c in columns)
    expert_rows = normalize(y_ref[...], ygain_ref[...]).astype(BF16)
    picked[...] = dot(jnp.transpose(choose)[:slots].astype(BF16), expert_rows).astype(BF16)
    swap = swap_matrix()
    for c in range(slots // 32):
        send[pl.ds(c * 512, 512), :] = to_wire(swap, picked[pl.ds(c * 32, 32), :])
    met()
    start, wait = exchange(send, land_ref, block, zs_sem, zr_sem)

    def spread(j):
        return pltpu.make_async_remote_copy(
            src_ref=normed.at[own],
            dst_ref=normed.at[own],
            send_sem=xs_sem.at[j],
            recv_sem=xr_sem.at[j],
            device_id={"tp": lax.rem(t + j, tp)},
            device_id_type=MESH,
        )

    start()
    for j in (1, tp - 1) + tuple(range(2, tp - 1)):
        spread(j).start()
    mine = pl.ds(pl.multiple_of(e * block, block), block)
    land_ref[mine, :] = send[mine, :]
    for load in loads:
        load.wait()
    for j in (0, 1, tp - 1) + tuple(range(2, tp - 1)):
        if j:
            spread(j).wait_recv()
        part = pl.ds(pl.multiple_of(lax.rem(t + tp - j, tp) * rows, rows), rows)
        block_rows = normed[part, :]
        q_ref[part, :] = dot(block_rows, weights[0]).astype(BF16)
        kv_ref[part, :head_width] = dot(block_rows, weights[1]).astype(BF16)
        kv_ref[part, head_width:] = dot(block_rows, weights[2]).astype(BF16)
    for j in range(1, tp):
        spread(j).wait_send()
    wait()


def second_kernel(
    pieces,
    land_ref, gate_ref, up_ref, down_ref,
    back_ref,
    gate, up, down, stack, sums, theirs, w_sem, xs_sem, xr_sem, ps_sem, pr_sem,
):
    tp, t = lax.axis_size("tp"), lax.axis_index("tp")
    slots = sums.shape[1]
    piece = slots // pieces
    loads = [
        pltpu.make_async_copy(w, v, w_sem.at[i])
        for i, (w, v) in enumerate(((gate_ref, gate), (up_ref, up), (down_ref, down)))
    ]
    for load in loads:
        load.start()
    met = greet(("tp",))
    swap = swap_matrix()
    order = (1, tp - 1) + tuple(range(2, tp - 1))

    def forth(j, c):
        return pltpu.make_async_remote_copy(
            src_ref=land_ref.at[pl.ds(c * piece * SUB, piece * SUB)],
            dst_ref=stack.at[j - 1, pl.ds(c * piece * SUB, piece * SUB)],
            send_sem=xs_sem.at[j - 1, c],
            recv_sem=xr_sem.at[j - 1, c],
            device_id={"tp": lax.rem(t + j, tp)},
            device_id_type=MESH,
        )

    def back(j, c):
        return pltpu.make_async_remote_copy(
            src_ref=sums.at[j, pl.ds(c * piece, piece)],
            dst_ref=theirs.at[j - 1, pl.ds(c * piece, piece)],
            send_sem=ps_sem.at[j - 1, c],
            recv_sem=pr_sem.at[j - 1, c],
            device_id={"tp": lax.rem(t + tp - j, tp)},
            device_id_type=MESH,
        )

    def expert(j, c):
        wire = land_ref if j == 0 else stack.at[j - 1]
        rows = jnp.concatenate(
            [
                from_wire(swap, wire[pl.ds((c * piece + 32 * i) * SUB, 32 * SUB), :])
                for i in range(piece // 32)
            ],
            axis=0,
        )
        gate_proj = dot(rows, gate[0])
        hidden = (gate_proj / (1.0 + jnp.exp(-gate_proj)) * dot(rows, up[0])).astype(BF16)
        sums[j, pl.ds(c * piece, piece), :] = dot(hidden, down[0]).astype(BF16)

    met()
    for c in range(pieces):
        for j in order:
            forth(j, c).start()
    for load in loads:
        load.wait()
    for c in range(pieces):
        expert(0, c)
    for c in range(pieces):
        for j in order:
            forth(j, c).wait_recv()
            expert(j, c)
            back(j, c).start()
    for c in range(pieces):
        for j in order:
            back(j, c).wait_recv()
        for i in range(piece // 32):
            here = pl.ds(c * piece + 32 * i, 32)
            total = sums[0, here, :].astype(F32)
            for j in range(1, tp):
                total = total + theirs[j - 1, here, :].astype(F32)
            back_ref[pl.ds((c * piece + 32 * i) * SUB, 32 * SUB), :] = to_wire(
                swap, total.astype(BF16)
            )
    for c in range(pieces):
        for j in order:
            forth(j, c).wait_send()
            back(j, c).wait_send()


def third_kernel(
    capacity,
    q_ref, all_ref, forget_ref, wo_ref, post_ref, back_ref, routes_ref, rweight_ref,
    mix_ref, out_ref,
    keys, running_max, running_sum, running_acc, attended, parts, theirs, returned, natural,
    k_sem, zs_sem, zr_sem, xs_sem, xr_sem,
):
    tp, t = lax.axis_size("tp"), lax.axis_index("tp")
    e = lax.axis_index("ep")
    span = q_ref.shape[0]
    rows, width = mix_ref.shape
    heads = forget_ref.shape[0]
    head_dim = q_ref.shape[1] // heads
    head_width = heads * head_dim
    slots = natural.shape[0]
    block = capacity * SUB
    scale = head_dim ** (-0.5) * LOG2E

    def load(j, slot):
        return pltpu.make_async_copy(
            all_ref.at[pl.ds(pl.multiple_of(j * span, span), span)], keys.at[slot], k_sem.at[slot]
        )

    load(0, 0).start()
    met = greet(("ep", "tp"))
    running_max[...] = jnp.full_like(running_max, MASKED)
    running_sum[...] = jnp.zeros_like(running_sum)
    running_acc[...] = jnp.zeros_like(running_acc)
    met()
    start, wait = exchange(back_ref, returned, block, zs_sem, zr_sem)
    start()
    mine = pl.ds(pl.multiple_of(e * block, block), block)
    returned[mine, :] = back_ref[mine, :]
    first = pl.multiple_of(e * span, span)
    base = forget_ref[:, pl.ds(first, LANE)][:, :1]

    def attend(j, slot, masked):
        bias = (base - forget_ref[:, pl.ds(pl.multiple_of(j * span, span), span)]) * LOG2E
        for h in range(heads):
            cols = slice(h * head_dim, (h + 1) * head_dim)
            vcols = slice(head_width + h * head_dim, head_width + (h + 1) * head_dim)
            scores = lax.dot_general(
                q_ref[:, cols], keys[slot, :, cols], (((1,), (1,)), ((), ())),
                preferred_element_type=F32,
            )
            scores = scores * scale + bias[h : h + 1, :]
            if masked:
                seen = lax.broadcasted_iota(jnp.int32, (span, span), 1) <= (
                    lax.broadcasted_iota(jnp.int32, (span, span), 0)
                )
                scores = jnp.where(seen, scores, MASKED)
            old = running_max[h]
            new = jnp.maximum(old, jnp.max(scores, axis=1, keepdims=True))
            weights = jnp.exp2(scores - jnp.tile(new, (1, span // LANE)))
            rescale = jnp.exp2(old - new)
            partial = weights[:, :LANE]
            for i in range(1, span // LANE):
                partial = partial + weights[:, i * LANE : (i + 1) * LANE]
            running_sum[h] = running_sum[h] * rescale + partial
            running_acc[h] = running_acc[h] * rescale + dot(weights.astype(BF16), keys[slot, :, vcols])
            running_max[h] = new

    @pl.loop(0, e)
    def _(j):
        slot = lax.rem(j, 2)
        load(j + 1, 1 - slot).start()
        load(j, slot).wait()
        attend(j, slot, False)

    last = lax.rem(e, 2)
    load(e, last).wait()
    attend(e, last, True)
    for h in range(heads):
        total = jnp.sum(running_sum[h], axis=1, keepdims=True)
        attended[:, h * head_dim : (h + 1) * head_dim] = (running_acc[h] / total).astype(BF16)

    def spread(j):
        return pltpu.make_async_remote_copy(
            src_ref=parts.at[j],
            dst_ref=theirs.at[j - 1],
            send_sem=xs_sem.at[j - 1],
            recv_sem=xr_sem.at[j - 1],
            device_id={"tp": lax.rem(t + j, tp)},
            device_id_type=MESH,
        )

    order = tuple(range(2, tp - 1)) + (1, tp - 1)
    for j in order + (0,):
        here = pl.ds(pl.multiple_of(lax.rem(t + j, tp) * rows, rows), rows)
        parts[j] = dot(attended[here, :], wo_ref[...]).astype(BF16)
        if j:
            spread(j).start()

    wait()
    swap = swap_matrix()
    for c in range(slots // 32):
        natural[pl.ds(c * 32, 32), :] = from_wire(swap, returned[pl.ds(c * 512, 512), :])
    columns = slot_columns(routes_ref[...], capacity)
    combined = jnp.zeros((rows, width), F32)
    for k, column in enumerate(columns):
        choose = chooser(column, slots).astype(BF16)
        combined = combined + rweight_ref[:, k : k + 1] * dot(choose, natural[...])
    out_ref[...] = combined.astype(BF16)

    total = parts[0].astype(F32)
    for j in range(1, tp):
        spread(j).wait_recv()
        total = total + theirs[j - 1].astype(F32)
    mix_ref[...] = normalize(total, post_ref[...]).astype(BF16)
    for j in range(1, tp):
        spread(j).wait_send()


def dma(*shape):
    return pltpu.SemaphoreType.DMA(shape)


def params(number):
    return pltpu.CompilerParams(
        collective_id=number, has_side_effects=True, vmem_limit_bytes=60 * 1024 * 1024
    )


def on_device(
    mixer_input, forget_cumsum, mixer_gain, query_weight, key_weight, value_weight, out_weight,
    post_gain, expert_input, expert_gain, routes, route_weight, expert_gate, expert_upward, expert_down,
):
    ep, tp = lax.axis_size("ep"), lax.axis_size("tp")
    rows, width = mixer_input.shape
    heads = forget_cumsum.shape[0]
    head_width = query_weight.shape[1]
    head_dim = head_width // heads
    span = rows * tp
    moe_rows, top = routes.shape
    experts = ep * expert_gate.shape[0]
    capacity = (moe_rows * top * 9 + 8 * experts - 1) // (8 * experts)
    slots = experts * capacity
    hidden = expert_gate.shape[2]
    wire = jax.ShapeDtypeStruct((slots * SUB, LANE), BF16)

    queries, pairs, arrived = pl.pallas_call(
        functools.partial(first_kernel, capacity),
        name="first",
        out_shape=(
            jax.ShapeDtypeStruct((span, head_width), BF16),
            jax.ShapeDtypeStruct((span, 2 * head_width), BF16),
            wire,
        ),
        in_specs=[VM, VM, ANY, ANY, ANY, VM, VM, VM],
        out_specs=(VM, VM, VM),
        scratch_shapes=[
            pltpu.VMEM((span, width), BF16),
            pltpu.VMEM((3, width, head_width), BF16),
            pltpu.VMEM((slots, width), BF16),
            pltpu.VMEM((slots * SUB, LANE), BF16),
            dma(3), dma(tp), dma(tp), dma(ep), dma(ep),
        ],
        compiler_params=params(0),
        cost_estimate=pl.CostEstimate(flops=4 * 10**9, bytes_accessed=10**8, transcendentals=0),
    )(
        mixer_input, mixer_gain[None], query_weight, key_weight, value_weight,
        expert_input, expert_gain[None], routes,
    )
    everyone = lax.all_gather(pairs, "ep", axis=0, tiled=True)

    pieces = 3
    back = pl.pallas_call(
        functools.partial(second_kernel, pieces),
        name="second",
        out_shape=wire,
        in_specs=[VM, ANY, ANY, ANY],
        out_specs=VM,
        scratch_shapes=[
            pltpu.VMEM((1, width, hidden), BF16),
            pltpu.VMEM((1, width, hidden), BF16),
            pltpu.VMEM((1, hidden, width), BF16),
            pltpu.VMEM((tp - 1, slots * SUB, LANE), BF16),
            pltpu.VMEM((tp, slots, width), BF16),
            pltpu.VMEM((tp - 1, slots, width), BF16),
            dma(3), dma(tp - 1, pieces), dma(tp - 1, pieces), dma(tp - 1, pieces), dma(tp - 1, pieces),
        ],
        compiler_params=params(1),
        cost_estimate=pl.CostEstimate(flops=8 * 10**9, bytes_accessed=2 * 10**8, transcendentals=0),
    )(arrived, expert_gate, expert_upward, expert_down)

    return pl.pallas_call(
        functools.partial(third_kernel, capacity),
        name="third",
        out_shape=(
            jax.ShapeDtypeStruct((rows, width), BF16),
            jax.ShapeDtypeStruct((moe_rows, width), BF16),
        ),
        in_specs=[VM, ANY, VM, VM, VM, VM, VM, VM],
        out_specs=(VM, VM),
        scratch_shapes=[
            pltpu.VMEM((2, span, 2 * head_width), BF16),
            pltpu.VMEM((heads, span, LANE), F32),
            pltpu.VMEM((heads, span, LANE), F32),
            pltpu.VMEM((heads, span, head_dim), F32),
            pltpu.VMEM((span, head_width), BF16),
            pltpu.VMEM((tp, rows, width), BF16),
            pltpu.VMEM((tp - 1, rows, width), BF16),
            pltpu.VMEM((slots * SUB, LANE), BF16),
            pltpu.VMEM((slots, width), BF16),
            dma(2), dma(ep), dma(ep), dma(tp - 1), dma(tp - 1),
        ],
        compiler_params=params(2),
        cost_estimate=pl.CostEstimate(flops=8 * 10**9, bytes_accessed=2 * 10**8, transcendentals=0),
    )(queries, everyone, forget_cumsum, out_weight, post_gain[None], back, routes, route_weight)


def solution(mesh):
    rows = P(("grp", "ep", "tp"), None)
    in_specs = (
        rows, P("tp", "grp"), P(), P(None, "tp"), P(None, "tp"), P(None, "tp"), P("tp", None), P(),
        rows, P(), rows, rows, P("ep", None, "tp"), P("ep", None, "tp"), P("ep", "tp", None),
    )
    return jax.shard_map(
        on_device, mesh=mesh, in_specs=in_specs, out_specs=(rows, rows), check_vma=False
    )
```

```python
import functools

import jax
import jax.numpy as jnp
from jax import lax
from jax.experimental import pallas as pl
from jax.experimental.pallas import tpu as pltpu
from jax.sharding import PartitionSpec as P

EPS = 1e-06
MASKED = -1e30
LOG2E = 1.4426950408889634
MESH = pl.DeviceIdType.MESH
SUB, LANE = 16, 128
BF16, F32 = jnp.bfloat16, jnp.float32
ANY = pl.BlockSpec(memory_space=pl.ANY)
VM = pl.BlockSpec(memory_space=pltpu.VMEM)


def normalize(row_block, gain):
    values = row_block.astype(F32)
    inverse = lax.rsqrt(jnp.mean(values * values, axis=-1, keepdims=True) + EPS)
    return values * inverse * gain


def dot(a, b):
    return jnp.dot(a, b, preferred_element_type=F32)


def swap_matrix():
    n = SUB * SUB
    i = lax.broadcasted_iota(jnp.int32, (n, n), 0)
    k = lax.broadcasted_iota(jnp.int32, (n, n), 1)
    hit = ((i // SUB) == (k % SUB)) & ((i % SUB) == (k // SUB))
    return jnp.where(hit, 1.0, 0.0).astype(BF16)


def to_wire(swap, rows):
    count = rows.shape[0] // SUB
    halves = [
        jnp.concatenate(
            [rows[SUB * a : SUB * (a + 1), LANE * s : LANE * (s + 1)] for s in range(SUB)], axis=0
        )
        for a in range(count)
    ]
    out = dot(swap, jnp.concatenate(halves, axis=1)).astype(BF16)
    return jnp.concatenate([out[:, LANE * a : LANE * (a + 1)] for a in range(count)], axis=0)


def from_wire(swap, tiles):
    n = SUB * SUB
    count = tiles.shape[0] // n
    out = dot(swap, jnp.concatenate([tiles[n * a : n * (a + 1)] for a in range(count)], axis=1))
    out = out.astype(BF16)
    halves = [
        jnp.concatenate(
            [out[SUB * s : SUB * (s + 1), LANE * a : LANE * (a + 1)] for s in range(SUB)], axis=1
        )
        for a in range(count)
    ]
    return jnp.concatenate(halves, axis=0)


def slot_columns(routes, capacity):
    rows, top = routes.shape
    experts = lax.broadcasted_iota(jnp.int32, (rows, LANE), 1)
    earlier = lax.broadcasted_iota(jnp.int32, (rows, rows), 1) < lax.broadcasted_iota(
        jnp.int32, (rows, rows), 0
    )
    earlier = jnp.where(earlier, 1.0, 0.0).astype(BF16)
    taken = jnp.zeros((1, LANE), F32)
    columns = []
    for k in range(top):
        member = jnp.where(experts == routes[:, k : k + 1], 1.0, 0.0)
        before = dot(earlier, member.astype(BF16)) + taken
        rank = jnp.sum(before * member, axis=1, keepdims=True)
        columns.append(routes[:, k : k + 1].astype(F32) * capacity + rank)
        taken = taken + jnp.sum(member, axis=0, keepdims=True)
    return columns


def chooser(column, width):
    ids = lax.broadcasted_iota(jnp.int32, (column.shape[0], width), 1).astype(F32)
    return jnp.where(ids == column, 1.0, 0.0)


def greet(axes):
    barrier = pltpu.get_barrier_semaphore()
    total = 0
    for axis in axes:
        n = lax.axis_size(axis)
        me = lax.axis_index(axis)

        @pl.loop(1, n)
        def _(s):
            pl.semaphore_signal(
                barrier, inc=1, device_id={axis: lax.rem(me + s, n)}, device_id_type=MESH
            )

        total += n - 1
    return lambda: pl.semaphore_wait(barrier, total)


def remote(src, dst, send_sem, recv_sem, **device):
    return pltpu.make_async_remote_copy(
        src_ref=src, dst_ref=dst, send_sem=send_sem, recv_sem=recv_sem,
        device_id=device, device_id_type=MESH,
    )


def aligned(start, size):
    return pl.ds(pl.multiple_of(start, size), size)


def kernel(
    capacity,
    x_ref, gain_ref, wq_ref, wk_ref, wv_ref, wo_ref, post_ref, forget_ref,
    y_ref, ygain_ref, routes_ref, rweight_ref, gate_ref, up_ref, down_ref,
    mix_ref, out_ref,
    normed, qkv_w, queries, keys, out_w, running_max, running_sum, running_acc, attended, parts, mix_theirs,
    natural, send, stack, gate, up, down, sums, theirs, back, returned,
    w_sem, ns_sem, nr_sem, zs_sem, zr_sem, gs_sem, gr_sem, ps_sem, pr_sem, bs_sem, br_sem, ms_sem, mr_sem,
    rs_sem, rr_sem, cs_sem, cr_sem,
):
    rows, width = x_ref.shape
    head_width = wq_ref.shape[1]
    heads = forget_ref.shape[0]
    head_dim = head_width // heads
    tp, t = lax.axis_size("tp"), lax.axis_index("tp")
    ep, e = lax.axis_size("ep"), lax.axis_index("ep")
    chips, chip, core = ep // 2, e // 2, lax.rem(e, 2)
    span = rows * tp
    slots = natural.shape[0]
    block = capacity * SUB
    pieces = 2
    piece = slots // pieces
    groups = 8
    group = ep // groups
    peers = (1, tp - 1) + tuple(range(2, tp - 1))

    loads = [
        pltpu.make_async_copy(src, dst, w_sem.at[i])
        for i, (src, dst) in enumerate(
            (
                (wq_ref, qkv_w.at[0]), (wk_ref, qkv_w.at[1]), (wv_ref, qkv_w.at[2]),
                (gate_ref, gate), (up_ref, up), (down_ref, down), (wo_ref, out_w),
            )
        )
    ]
    for load in loads:
        load.start()
    met = greet(("ep", "tp"))

    columns = slot_columns(routes_ref[...], capacity)
    padded = -(-slots // LANE) * LANE
    choose = sum(chooser(c, padded) for c in columns)
    expert_rows = normalize(y_ref[...], ygain_ref[...]).astype(BF16)
    natural[...] = dot(jnp.transpose(choose)[:slots].astype(BF16), expert_rows).astype(BF16)
    swap = swap_matrix()
    for c in range(slots // 32):
        send[pl.ds(c * 512, 512), :] = to_wire(swap, natural[pl.ds(c * 32, 32), :])
    met()

    def offset(p):
        return lax.rem(p, 2) * ((p + 1) // 2) + (1 - lax.rem(p, 2)) * (ep - p // 2)

    def dispatch(p):
        to = lax.rem(e + offset(p), ep)
        return remote(
            send.at[aligned(to * block, block)], stack.at[0, aligned(p * block, block)],
            zs_sem.at[p], zr_sem.at[p], ep=to,
        )

    @pl.loop(1, ep)
    def _(p):
        dispatch(p).start()

    stack[0, :block, :] = send[aligned(e * block, block), :]

    own = aligned(t * rows, rows)
    normed[own, :] = normalize(x_ref[...], gain_ref[...]).astype(BF16)

    def spread(j):
        return remote(
            normed.at[own], normed.at[own], ns_sem.at[j - 1], nr_sem.at[j - 1], tp=lax.rem(t + j, tp)
        )

    for j in peers:
        spread(j).start()
    running_max[...] = jnp.full_like(running_max, MASKED)
    running_sum[...] = jnp.zeros_like(running_sum)
    running_acc[...] = jnp.zeros_like(running_acc)
    for load in loads:
        load.wait()
    for j in (0,) + peers:
        if j:
            spread(j).wait_recv()
        part = aligned(lax.rem(t + tp - j, tp) * rows, rows)
        block_rows = normed[part, :]
        queries[part, :] = dot(block_rows, qkv_w[0]).astype(BF16)
        for half in range(2):
            keys[e, half, part, :] = dot(block_rows, qkv_w[1 + half]).astype(BF16)

    def source(way, h):
        return lax.rem(chip + (chips - h if way == 0 else h), chips)

    def hop(way, half, h):
        at = 2 * source(way, h - 1) + core
        to = lax.rem(e + (2 if way == 0 else ep - 2), ep)
        return remote(
            keys.at[at, half], keys.at[at, half], rs_sem.at[way, half, h], rr_sem.at[way, half, h], ep=to
        )

    def share(way, half, h):
        at = 2 * source(way, h) + core
        return remote(
            keys.at[at, half], keys.at[at, half], cs_sem.at[way, half, h], cr_sem.at[way, half, h],
            ep=e + 1 - 2 * core,
        )

    def farthest(way, half):
        return chips // 2 if way == half else chips // 2 - 1

    def comes(way, half, h):
        near = h <= farthest(way, half)
        return near & (chip >= h if way == 0 else lax.rem(chip + h, chips) < chips // 2)

    def needed(way, half, h):
        return (h <= farthest(way, half)) & (chip >= h if way == 0 else chip + h >= chips)

    def goes(way, half, h):
        near = h <= farthest(way, half)
        if way == 0:
            return near & (chip >= h - 1) & (chip + 1 < chips)
        return near & (lax.rem(chip + h - 1, chips) < chips // 2)

    WAYS = [(way, half) for half in range(2) for way in range(2)]
    for way, half in WAYS:
        @pl.when(goes(way, half, 1))
        def _():
            hop(way, half, 1).start()

    for half in range(2):
        share(0, half, 0).start()

    def forth(j, g):
        size = group * block
        return remote(
            stack.at[0, aligned(g * size, size)], stack.at[j, aligned(g * size, size)],
            gs_sem.at[j - 1, g], gr_sem.at[j - 1, g], tp=lax.rem(t + j, tp),
        )

    def back_to(j, p):
        return remote(
            sums.at[j, aligned(p * piece, piece)], theirs.at[j - 1, aligned(p * piece, piece)],
            ps_sem.at[j - 1, p], pr_sem.at[j - 1, p], tp=lax.rem(t + tp - j, tp),
        )

    def expert(j, p):
        tiles = piece * SUB
        half_tiles = 256 * (piece // SUB // 2)
        start = p * tiles
        got = [
            from_wire(swap, stack[j, pl.ds(pl.multiple_of(start + at, 256), size), :])
            for at, size in ((0, half_tiles), (half_tiles, tiles - half_tiles))
        ]
        batch = jnp.concatenate(got, axis=0)
        gate_proj = dot(batch, gate[0])
        hidden = (gate_proj / (1.0 + jnp.exp(-gate_proj)) * dot(batch, up[0])).astype(BF16)
        sums[j, aligned(p * piece, piece), :] = dot(hidden, down[0]).astype(BF16)

    @pl.loop(0, groups)
    def _(g):
        @pl.loop(0, group)
        def _(i):
            @pl.when(g * group + i > 0)
            def _():
                dispatch(g * group + i).wait_recv()

        for j in peers:
            forth(j, g).start()

    @pl.loop(0, pieces)
    def _(p):
        expert(0, p)

    def serve(p):
        @pl.loop(1, tp)
        def _(i):
            j = i + (i // 2) * (1 - 2 * lax.rem(i, 2))

            @pl.loop(0, groups // pieces)
            def _(g):
                forth(j, p * (groups // pieces) + g).wait_recv()

            expert(j, p)
            back_to(j, p).start()

    def give_back(p):
        from_here = lax.rem(e + ep - offset(p), ep)
        return remote(
            back.at[aligned(p * block, block)], returned.at[aligned(e * block, block)],
            bs_sem.at[p], br_sem.at[p], ep=from_here,
        )

    def reduce(p):
        for j in peers:
            back_to(j, p).wait_recv()

        @pl.loop(0, piece // SUB)
        def _(i):
            here = pl.ds(pl.multiple_of(p * piece + SUB * i, SUB), SUB)
            total = sums[0, here, :].astype(F32)
            for j in range(1, tp):
                total = total + theirs[j - 1, here, :].astype(F32)
            back[pl.ds(pl.multiple_of((p * piece + SUB * i) * SUB, 256), 256), :] = to_wire(
                swap, total.astype(BF16)
            )

        @pl.loop(0, ep // pieces)
        def _(i):
            @pl.when(p * (ep // pieces) + i > 0)
            def _():
                give_back(p * (ep // pieces) + i).start()

    scale = head_dim ** (-0.5) * LOG2E
    base = forget_ref[:, aligned(e * span, span)][:, :1]

    def attend(j, masked):
        bias = (base - forget_ref[:, aligned(j * span, span)]) * LOG2E
        for h in range(heads):
            cols = slice(h * head_dim, (h + 1) * head_dim)
            scores = lax.dot_general(
                queries[:, cols], keys[j, 0, :, cols], (((1,), (1,)), ((), ())),
                preferred_element_type=F32,
            )
            scores = scores * scale + bias[h : h + 1, :]
            if masked:
                seen = lax.broadcasted_iota(jnp.int32, (span, span), 1) <= (
                    lax.broadcasted_iota(jnp.int32, (span, span), 0)
                )
                scores = jnp.where(seen, scores, MASKED)
            old = running_max[h]
            new = jnp.maximum(old, jnp.max(scores, axis=1, keepdims=True))
            weights = jnp.exp2(scores - jnp.tile(new, (1, span // LANE)))
            rescale = jnp.exp2(old - new)
            partial = weights[:, :LANE]
            for i in range(1, span // LANE):
                partial = partial + weights[:, i * LANE : (i + 1) * LANE]
            running_sum[h] = running_sum[h] * rescale + partial
            running_acc[h] = running_acc[h] * rescale + dot(weights.astype(BF16), keys[j, 1, :, cols])
            running_max[h] = new

    attend(e, True)
    last = chips // 2

    @pl.loop(1, last + 2)
    def _(h):
        for way, half in WAYS:
            @pl.when(comes(way, half, h))
            def _():
                hop(way, half, h).wait_recv()

                @pl.when(goes(way, half, h + 1))
                def _():
                    hop(way, half, h + 1).start()

                @pl.when(needed(way, half, h))
                def _():
                    share(way, half, h).start()

        g = h - 1
        for way, half in WAYS:
            @pl.when(needed(way, half, g) if way == 0 else needed(way, half, g) & (g > 0))
            def _():
                share(way, half, g).wait_recv()

        @pl.loop(0, 4)
        def _(i):
            side, parity = i // 2, lax.rem(i, 2)
            away = (g > 0) & (
                ((side == 0) & (chip >= g)) | ((side == 1) & (chip + g >= chips) & (g < last))
            )
            home = (g == 0) & (i == 0) & (core == 1)

            @pl.when(away | home)
            def _():
                attend(2 * (chip - g + side * (2 * g - chips)) + parity, False)

        @pl.when((h == 2) | (h == 4))
        def _():
            serve(h // 2 - 1)

        @pl.when((h == 6) | (h == 8))
        def _():
            reduce(h // 2 - 3)

    for h in range(heads):
        total = jnp.sum(running_sum[h], axis=1, keepdims=True)
        attended[:, h * head_dim : (h + 1) * head_dim] = (running_acc[h] / total).astype(BF16)

    def mix_to(j):
        return remote(
            parts.at[j], mix_theirs.at[j - 1], ms_sem.at[j - 1], mr_sem.at[j - 1], tp=lax.rem(t + j, tp)
        )

    for j in tuple(range(2, tp - 1)) + (1, tp - 1, 0):
        here = aligned(lax.rem(t + j, tp) * rows, rows)
        parts[j] = dot(attended[here, :], out_w[...]).astype(BF16)
        if j:
            mix_to(j).start()

    returned[aligned(e * block, block), :] = back[:block, :]

    @pl.loop(1, ep)
    def _(p):
        give_back(p).wait_recv()

    for c in range(slots // 32):
        natural[pl.ds(c * 32, 32), :] = from_wire(swap, returned[pl.ds(c * 512, 512), :])
    columns = slot_columns(routes_ref[...], capacity)
    combined = jnp.zeros((rows, width), F32)
    for k, column in enumerate(columns):
        chosen = chooser(column, slots).astype(BF16)
        combined = combined + rweight_ref[:, k : k + 1] * dot(chosen, natural[...])
    out_ref[...] = combined.astype(BF16)

    total = parts[0].astype(F32)
    for j in range(1, tp):
        mix_to(j).wait_recv()
        total = total + mix_theirs[j - 1].astype(F32)
    mix_ref[...] = normalize(total, post_ref[...]).astype(BF16)

    for j in range(1, tp):
        spread(j).wait_send()
        mix_to(j).wait_send()
        for p in range(pieces):
            back_to(j, p).wait_send()

        @pl.loop(0, groups)
        def _(g):
            forth(j, g).wait_send()

    @pl.loop(1, ep)
    def _(p):
        dispatch(p).wait_send()
        give_back(p).wait_send()

    for half in range(2):
        share(0, half, 0).wait_send()

    @pl.loop(1, last + 1)
    def _(h):
        for way, half in WAYS:
            @pl.when(goes(way, half, h))
            def _():
                hop(way, half, h).wait_send()

            @pl.when(needed(way, half, h))
            def _():
                share(way, half, h).wait_send()


def dma(*shape):
    return pltpu.SemaphoreType.DMA(shape)


def on_device(
    mixer_input, forget_cumsum, mixer_gain, query_weight, key_weight, value_weight, out_weight,
    post_gain, expert_input, expert_gain, routes, route_weight, expert_gate, expert_upward, expert_down,
):
    ep, tp = lax.axis_size("ep"), lax.axis_size("tp")
    rows, width = mixer_input.shape
    heads = forget_cumsum.shape[0]
    head_width = query_weight.shape[1]
    head_dim = head_width // heads
    span = rows * tp
    moe_rows, top = routes.shape
    experts = ep * expert_gate.shape[0]
    capacity = (moe_rows * top * 9 + 8 * experts - 1) // (8 * experts)
    slots = experts * capacity
    hidden = expert_gate.shape[2]
    vmem = pltpu.VMEM
    hops = ep // 4 + 3

    return pl.pallas_call(
        functools.partial(kernel, capacity),
        name="block",
        out_shape=(
            jax.ShapeDtypeStruct((rows, width), BF16),
            jax.ShapeDtypeStruct((moe_rows, width), BF16),
        ),
        in_specs=[VM, VM, ANY, ANY, ANY, ANY, VM, VM, VM, VM, VM, VM, ANY, ANY, ANY],
        out_specs=(VM, VM),
        scratch_shapes=[
            vmem((span, width), BF16),
            vmem((3, width, head_width), BF16),
            vmem((span, head_width), BF16),
            vmem((ep, 2, span, head_width), BF16),
            vmem((head_width, width), BF16),
            vmem((heads, span, LANE), F32),
            vmem((heads, span, LANE), F32),
            vmem((heads, span, head_dim), F32),
            vmem((span, head_width), BF16),
            vmem((tp, rows, width), BF16),
            vmem((tp - 1, rows, width), BF16),
            vmem((slots, width), BF16),
            vmem((slots * SUB, LANE), BF16),
            vmem((tp, slots * SUB, LANE), BF16),
            vmem((1, width, hidden), BF16),
            vmem((1, width, hidden), BF16),
            vmem((1, hidden, width), BF16),
            vmem((tp, slots, width), BF16),
            vmem((tp - 1, slots, width), BF16),
            vmem((slots * SUB, LANE), BF16),
            vmem((slots * SUB, LANE), BF16),
            dma(7), dma(tp - 1), dma(tp - 1), dma(ep), dma(ep), dma(tp - 1, 8), dma(tp - 1, 8),
            dma(tp - 1, 2), dma(tp - 1, 2), dma(ep), dma(ep), dma(tp - 1), dma(tp - 1),
            dma(2, 2, hops), dma(2, 2, hops), dma(2, 2, hops), dma(2, 2, hops),
        ],
        compiler_params=pltpu.CompilerParams(
            collective_id=0, has_side_effects=True, vmem_limit_bytes=63 * 1024 * 1024
        ),
    )(
        mixer_input, mixer_gain[None], query_weight, key_weight, value_weight, out_weight,
        post_gain[None], forget_cumsum, expert_input, expert_gain[None], routes, route_weight,
        expert_gate, expert_upward, expert_down,
    )


def solution(mesh):
    rows = P(("grp", "ep", "tp"), None)
    in_specs = (
        rows, P("tp", "grp"), P(), P(None, "tp"), P(None, "tp"), P(None, "tp"), P("tp", None), P(),
        rows, P(), rows, rows, P("ep", None, "tp"), P("ep", None, "tp"), P("ep", "tp", None),
    )
    return jax.shard_map(
        on_device, mesh=mesh, in_specs=in_specs, out_specs=(rows, rows), check_vma=False
    )
```

```python
import functools

import jax
import jax.numpy as jnp
from jax import lax
from jax.experimental import pallas as pl
from jax.experimental.pallas import tpu as pltpu
from jax.sharding import PartitionSpec as P

EPS = 1e-06
MASKED = -1e30
LOG2E = 1.4426950408889634
MESH = pl.DeviceIdType.MESH
SUB, LANE = 16, 128
TOP = 2
SERVE = ((0, 0), (1, 5))
REDUCE = ((0, 9), (1, 13))
BF16, F32 = jnp.bfloat16, jnp.float32
ANY = pl.BlockSpec(memory_space=pl.ANY)
VM = pl.BlockSpec(memory_space=pltpu.VMEM)


def normalize(row_block, gain):
    values = row_block.astype(F32)
    inverse = lax.rsqrt(jnp.mean(values * values, axis=-1, keepdims=True) + EPS)
    return values * inverse * gain


def dot(a, b):
    return jnp.dot(a, b, preferred_element_type=F32)


def swap_matrix():
    n = SUB * SUB
    i = lax.broadcasted_iota(jnp.int32, (n, n), 0)
    k = lax.broadcasted_iota(jnp.int32, (n, n), 1)
    hit = ((i // SUB) == (k % SUB)) & ((i % SUB) == (k // SUB))
    return jnp.where(hit, 1.0, 0.0).astype(BF16)


def to_wire(swap, rows):
    count = rows.shape[0] // SUB
    halves = [
        jnp.concatenate(
            [rows[SUB * a : SUB * (a + 1), LANE * s : LANE * (s + 1)] for s in range(SUB)], axis=0
        )
        for a in range(count)
    ]
    out = dot(swap, jnp.concatenate(halves, axis=1)).astype(BF16)
    return jnp.concatenate([out[:, LANE * a : LANE * (a + 1)] for a in range(count)], axis=0)


def from_wire(swap, tiles):
    n = SUB * SUB
    count = tiles.shape[0] // n
    out = dot(swap, jnp.concatenate([tiles[n * a : n * (a + 1)] for a in range(count)], axis=1))
    out = out.astype(BF16)
    halves = [
        jnp.concatenate(
            [out[SUB * s : SUB * (s + 1), LANE * a : LANE * (a + 1)] for s in range(SUB)], axis=1
        )
        for a in range(count)
    ]
    return jnp.concatenate(halves, axis=0)


def upright(ref):
    top, rows = ref.shape
    return jnp.transpose(
        jnp.concatenate([ref[...].astype(F32), jnp.zeros((8 - top, rows), F32)], axis=0)
    )


def slot_columns(routes, capacity):
    rows, top = routes.shape[0], TOP
    experts = lax.broadcasted_iota(jnp.int32, (rows, LANE), 1).astype(F32)
    earlier = lax.broadcasted_iota(jnp.int32, (rows, rows), 1) < lax.broadcasted_iota(
        jnp.int32, (rows, rows), 0
    )
    earlier = jnp.where(earlier, 1.0, 0.0).astype(BF16)
    taken = jnp.zeros((1, LANE), F32)
    columns = []
    for k in range(top):
        member = jnp.where(experts == routes[:, k : k + 1], 1.0, 0.0)
        before = dot(earlier, member.astype(BF16)) + taken
        rank = jnp.sum(before * member, axis=1, keepdims=True)
        columns.append(routes[:, k : k + 1] * capacity + rank)
        taken = taken + jnp.sum(member, axis=0, keepdims=True)
    return columns


def chooser(column, width):
    ids = lax.broadcasted_iota(jnp.int32, (column.shape[0], width), 1).astype(F32)
    return jnp.where(ids == column, 1.0, 0.0)


def greet(axes):
    barrier = pltpu.get_barrier_semaphore()
    total = 0
    for axis in axes:
        n = lax.axis_size(axis)
        me = lax.axis_index(axis)

        @pl.loop(1, n)
        def _(s):
            pl.semaphore_signal(
                barrier, inc=1, device_id={axis: lax.rem(me + s, n)}, device_id_type=MESH
            )

        total += n - 1
    return lambda: pl.semaphore_wait(barrier, total)


def remote(src, dst, send_sem, recv_sem, **device):
    return pltpu.make_async_remote_copy(
        src_ref=src, dst_ref=dst, send_sem=send_sem, recv_sem=recv_sem,
        device_id=device, device_id_type=MESH,
    )


def aligned(start, size):
    return pl.ds(pl.multiple_of(start, size), size)


def attend_block(queries, pair, bias, running_max, running_sum, running_acc, masked):
    heads, span, head_dim = running_acc.shape
    scale = head_dim ** (-0.5) * LOG2E
    for h in range(heads):
        cols = slice(h * head_dim, (h + 1) * head_dim)
        scores = lax.dot_general(
            queries[:, cols], pair[0, :, cols], (((1,), (1,)), ((), ())), preferred_element_type=F32
        )
        scores = scores * scale + bias[h : h + 1, :]
        if masked:
            seen = lax.broadcasted_iota(jnp.int32, (span, span), 1) <= (
                lax.broadcasted_iota(jnp.int32, (span, span), 0)
            )
            scores = jnp.where(seen, scores, MASKED)
        old = running_max[h]
        new = jnp.maximum(old, jnp.max(scores, axis=1, keepdims=True))
        weights = jnp.exp2(scores - jnp.tile(new, (1, span // LANE)))
        rescale = jnp.exp2(old - new)
        partial = weights[:, :LANE]
        for i in range(1, span // LANE):
            partial = partial + weights[:, i * LANE : (i + 1) * LANE]
        running_sum[h] = running_sum[h] * rescale + partial
        running_acc[h] = running_acc[h] * rescale + dot(weights.astype(BF16), pair[1, :, cols])
        running_max[h] = new


def expert_block(swap, stack, gate, up, down, sums, start, piece):
    tiles = piece * SUB
    half_tiles = 256 * (piece // SUB // 2)
    got = [
        from_wire(swap, stack[pl.ds(pl.multiple_of(start * SUB + at, 256), size), :])
        for at, size in ((0, half_tiles), (half_tiles, tiles - half_tiles))
    ]
    batch = jnp.concatenate(got, axis=0)
    gate_proj = dot(batch, gate[0])
    hidden = (gate_proj / (1.0 + jnp.exp(-gate_proj)) * dot(batch, up[0])).astype(BF16)
    sums[aligned(start, piece), :] = dot(hidden, down[0]).astype(BF16)


def kernel(
    capacity,
    x_ref, gain_ref, wq_ref, wk_ref, wv_ref, wo_ref, post_ref, forget_ref,
    y_ref, ygain_ref, routes_ref, rweight_ref, gate_ref, up_ref, down_ref,
    mix_ref, out_ref,
    normed, qkv_w, queries, keys, out_w, running_max, running_sum, running_acc, attended, parts, mix_theirs,
    natural, send, stack, gate, up, down, sums, theirs, back, returned,
    w_sem, ns_sem, nr_sem, zs_sem, zr_sem, gs_sem, gr_sem, ps_sem, pr_sem, bs_sem, br_sem, ms_sem, mr_sem,
    rs_sem, rr_sem, cs_sem, cr_sem,
):
    rows, width = x_ref.shape
    head_width = wq_ref.shape[1]
    heads = forget_ref.shape[0]
    head_dim = head_width // heads
    tp, t = lax.axis_size("tp"), lax.axis_index("tp")
    ep, e = lax.axis_size("ep"), lax.axis_index("ep")
    chips, chip, core = ep // 2, e // 2, lax.rem(e, 2)
    span = rows * tp
    slots = natural.shape[0]
    block = capacity * SUB
    pieces = 2
    piece = slots // pieces
    groups = 8
    group = ep // groups
    peers = (1, tp - 1) + tuple(range(2, tp - 1))

    loads = [
        pltpu.make_async_copy(src, dst, w_sem.at[i])
        for i, (src, dst) in enumerate(
            (
                (wq_ref, qkv_w.at[0]), (wk_ref, qkv_w.at[1]), (wv_ref, qkv_w.at[2]),
                (gate_ref, gate), (up_ref, up), (down_ref, down), (wo_ref, out_w),
            )
        )
    ]
    for load in loads:
        load.start()
    met = greet(("ep", "tp"))

    columns = slot_columns(upright(routes_ref), capacity)
    padded = -(-slots // LANE) * LANE
    choose = sum(chooser(c, padded) for c in columns)
    expert_rows = normalize(y_ref[...], ygain_ref[...]).astype(BF16)
    natural[...] = dot(jnp.transpose(choose)[:slots].astype(BF16), expert_rows).astype(BF16)
    swap = swap_matrix()
    for c in range(slots // 32):
        send[pl.ds(c * 512, 512), :] = to_wire(swap, natural[pl.ds(c * 32, 32), :])
    met()

    def offset(p):
        return lax.rem(p, 2) * ((p + 1) // 2) + (1 - lax.rem(p, 2)) * (ep - p // 2)

    def dispatch(p):
        to = lax.rem(e + offset(p), ep)
        return remote(
            send.at[aligned(to * block, block)], stack.at[0, aligned(p * block, block)],
            zs_sem.at[p], zr_sem.at[p], ep=to,
        )

    @pl.loop(1, ep)
    def _(p):
        dispatch(p).start()

    stack[0, :block, :] = send[aligned(e * block, block), :]

    own = aligned(t * rows, rows)
    normed[own, :] = normalize(x_ref[...], gain_ref[...]).astype(BF16)

    def spread(j):
        return remote(
            normed.at[own], normed.at[own], ns_sem.at[j - 1], nr_sem.at[j - 1], tp=lax.rem(t + j, tp)
        )

    for j in peers:
        spread(j).start()
    running_max[...] = jnp.full_like(running_max, MASKED)
    running_sum[...] = jnp.zeros_like(running_sum)
    running_acc[...] = jnp.zeros_like(running_acc)
    for load in loads:
        load.wait()
    for j in (0,) + peers:
        if j:
            spread(j).wait_recv()
        part = aligned(lax.rem(t + tp - j, tp) * rows, rows)
        block_rows = normed[part, :]
        queries[part, :] = dot(block_rows, qkv_w[0]).astype(BF16)
        for half in range(2):
            keys[e, half, part, :] = dot(block_rows, qkv_w[1 + half]).astype(BF16)

    def source(way, h):
        return lax.rem(chip + (chips - h if way == 0 else h), chips)

    def hop(way, half, h):
        at = 2 * source(way, h - 1) + core
        to = lax.rem(e + (2 if way == 0 else ep - 2), ep)
        return remote(
            keys.at[at, half], keys.at[at, half], rs_sem.at[way, half, h], rr_sem.at[way, half, h], ep=to
        )

    def share(way, half, h):
        at = 2 * source(way, h) + core
        return remote(
            keys.at[at, half], keys.at[at, half], cs_sem.at[way, half, h], cr_sem.at[way, half, h],
            ep=e + 1 - 2 * core,
        )

    def farthest(way, half):
        return chips // 2 if way == half else chips // 2 - 1

    def comes(way, half, h):
        near = h <= farthest(way, half)
        return near & (chip >= h if way == 0 else lax.rem(chip + h, chips) < chips // 2)

    def needed(way, half, h):
        return (h <= farthest(way, half)) & (chip >= h if way == 0 else chip + h >= chips)

    def goes(way, half, h):
        near = h <= farthest(way, half)
        if way == 0:
            return near & (chip >= h - 1) & (chip + 1 < chips)
        return near & (lax.rem(chip + h - 1, chips) < chips // 2)

    WAYS = [(way, half) for half in range(2) for way in range(2)]
    for way, half in WAYS:
        @pl.when(goes(way, half, 1))
        def _():
            hop(way, half, 1).start()

    for half in range(2):
        share(0, half, 0).start()

    def forth(j, g):
        size = group * block
        return remote(
            stack.at[0, aligned(g * size, size)], stack.at[j, aligned(g * size, size)],
            gs_sem.at[j - 1, g], gr_sem.at[j - 1, g], tp=lax.rem(t + j, tp),
        )

    def back_to(j, p):
        return remote(
            sums.at[j, aligned(p * piece, piece)], theirs.at[j - 1, aligned(p * piece, piece)],
            ps_sem.at[j - 1, p], pr_sem.at[j - 1, p], tp=lax.rem(t + tp - j, tp),
        )

    def expert(j, p):
        expert_block(swap, stack.at[j], gate, up, down, sums.at[j], p * piece, piece)

    @pl.loop(0, groups)
    def _(g):
        @pl.loop(0, group)
        def _(i):
            @pl.when(g * group + i > 0)
            def _():
                dispatch(g * group + i).wait_recv()

        for j in peers:
            forth(j, g).start()

    @pl.loop(0, pieces)
    def _(p):
        expert(0, p)

    def serve(i, p):
        j = i + (i // 2) * (1 - 2 * (i % 2))

        @pl.loop(0, groups // pieces)
        def _(g):
            forth(j, p * (groups // pieces) + g).wait_recv()

        expert(j, p)
        back_to(j, p).start()

    def give_back(p):
        from_here = lax.rem(e + ep - offset(p), ep)
        return remote(
            back.at[aligned(p * block, block)], returned.at[aligned(e * block, block)],
            bs_sem.at[p], br_sem.at[p], ep=from_here,
        )

    def reduce(p):
        for j in peers:
            back_to(j, p).wait_recv()

        @pl.loop(0, piece // SUB)
        def _(i):
            here = pl.ds(pl.multiple_of(p * piece + SUB * i, SUB), SUB)
            total = sums[0, here, :].astype(F32)
            for j in range(1, tp):
                total = total + theirs[j - 1, here, :].astype(F32)
            back[pl.ds(pl.multiple_of((p * piece + SUB * i) * SUB, 256), 256), :] = to_wire(
                swap, total.astype(BF16)
            )

        @pl.loop(0, ep // pieces)
        def _(i):
            @pl.when(p * (ep // pieces) + i > 0)
            def _():
                give_back(p * (ep // pieces) + i).start()

    base = forget_ref[:, aligned(e * span, span)][:, :1]

    def attend(j, masked):
        bias = (base - forget_ref[:, aligned(j * span, span)]) * LOG2E
        attend_block(
            queries, keys.at[j], bias, running_max, running_sum, running_acc, masked
        )

    attend(e, True)
    last = chips // 2

    def pump(half, h):
        for way in range(2):
            @pl.when(comes(way, half, h))
            def _():
                hop(way, half, h).wait_recv()

                @pl.when(goes(way, half, h + 1))
                def _():
                    hop(way, half, h + 1).start()

                @pl.when(needed(way, half, h))
                def _():
                    share(way, half, h).start()

    @pl.loop(0, 2 * last + 2)
    def _(u):
        h, half = u // 2 + 1, lax.rem(u, 2)
        g = h - 1
        for which in range(2):
            @pl.when(half == which)
            def _():
                pump(which, h)

        @pl.when(half == 0)
        def _():
            for way, what in WAYS:
                @pl.when(needed(way, what, g))
                def _():
                    share(way, what, g).wait_recv()

        @pl.loop(0, 2)
        def _(parity):
            away = (g > 0) & (
                ((half == 0) & (chip >= g)) | ((half == 1) & (chip + g >= chips) & (g < last))
            )
            home = (u == 0) & (parity == 0) & (core == 1)

            @pl.when(away | home)
            def _():
                attend(2 * (chip - g + half * (2 * g - chips)) + parity, False)

        for p, first in SERVE:
            for i in range(1, tp):
                @pl.when(u == first + i - 1)
                def _():
                    serve(i, p)

        for p, at in REDUCE:
            @pl.when(u == at)
            def _():
                reduce(p)

    for h in range(heads):
        total = jnp.sum(running_sum[h], axis=1, keepdims=True)
        attended[:, h * head_dim : (h + 1) * head_dim] = (running_acc[h] / total).astype(BF16)

    def mix_to(j):
        return remote(
            parts.at[j], mix_theirs.at[j - 1], ms_sem.at[j - 1], mr_sem.at[j - 1], tp=lax.rem(t + j, tp)
        )

    for j in tuple(range(2, tp - 1)) + (1, tp - 1, 0):
        here = aligned(lax.rem(t + j, tp) * rows, rows)
        parts[j] = dot(attended[here, :], out_w[...]).astype(BF16)
        if j:
            mix_to(j).start()

    returned[aligned(e * block, block), :] = back[:block, :]

    @pl.loop(1, ep)
    def _(p):
        give_back(p).wait_recv()

    for c in range(slots // 32):
        natural[pl.ds(c * 32, 32), :] = from_wire(swap, returned[pl.ds(c * 512, 512), :])
    columns = slot_columns(upright(routes_ref), capacity)
    combined = jnp.zeros((rows, width), F32)
    rweight = upright(rweight_ref)
    for k, column in enumerate(columns):
        chosen = chooser(column, slots).astype(BF16)
        combined = combined + rweight[:, k : k + 1] * dot(chosen, natural[...])
    out_ref[...] = combined.astype(BF16)

    total = parts[0].astype(F32)
    for j in range(1, tp):
        mix_to(j).wait_recv()
        total = total + mix_theirs[j - 1].astype(F32)
    mix_ref[...] = normalize(total, post_ref[...]).astype(BF16)

    for j in range(1, tp):
        spread(j).wait_send()
        mix_to(j).wait_send()
        for p in range(pieces):
            back_to(j, p).wait_send()

        @pl.loop(0, groups)
        def _(g):
            forth(j, g).wait_send()

    @pl.loop(1, ep)
    def _(p):
        dispatch(p).wait_send()
        give_back(p).wait_send()

    for half in range(2):
        share(0, half, 0).wait_send()

    @pl.loop(1, last + 1)
    def _(h):
        for way, half in WAYS:
            @pl.when(goes(way, half, h))
            def _():
                hop(way, half, h).wait_send()

            @pl.when(needed(way, half, h))
            def _():
                share(way, half, h).wait_send()


def hand_over(mix_ref, out_ref, mix_result, out_result):
    mix_result[...] = mix_ref[...]
    out_result[...] = out_ref[...]


def dma(*shape):
    return pltpu.SemaphoreType.DMA(shape)


def on_device(
    mixer_input, forget_cumsum, mixer_gain, query_weight, key_weight, value_weight, out_weight,
    post_gain, expert_input, expert_gain, routes, route_weight, expert_gate, expert_upward, expert_down,
):
    ep, tp = lax.axis_size("ep"), lax.axis_size("tp")
    rows, width = mixer_input.shape
    heads = forget_cumsum.shape[0]
    head_width = query_weight.shape[1]
    head_dim = head_width // heads
    span = rows * tp
    moe_rows, top = routes.shape
    experts = ep * expert_gate.shape[0]
    capacity = (moe_rows * top * 9 + 8 * experts - 1) // (8 * experts)
    slots = experts * capacity
    hidden = expert_gate.shape[2]
    vmem = pltpu.VMEM
    hops = ep // 4 + 3

    results = pl.pallas_call(
        functools.partial(kernel, capacity),
        name="block",
        out_shape=(
            jax.ShapeDtypeStruct((rows, width), BF16),
            jax.ShapeDtypeStruct((moe_rows, width), BF16),
        ),
        in_specs=[VM, VM, ANY, ANY, ANY, ANY, VM, VM, VM, VM, VM, VM, ANY, ANY, ANY],
        out_specs=(VM, VM),
        scratch_shapes=[
            vmem((span, width), BF16),
            vmem((3, width, head_width), BF16),
            vmem((span, head_width), BF16),
            vmem((ep, 2, span, head_width), BF16),
            vmem((head_width, width), BF16),
            vmem((heads, span, LANE), F32),
            vmem((heads, span, LANE), F32),
            vmem((heads, span, head_dim), F32),
            vmem((span, head_width), BF16),
            vmem((tp, rows, width), BF16),
            vmem((tp - 1, rows, width), BF16),
            vmem((slots, width), BF16),
            vmem((slots * SUB, LANE), BF16),
            vmem((tp, slots * SUB, LANE), BF16),
            vmem((1, width, hidden), BF16),
            vmem((1, width, hidden), BF16),
            vmem((1, hidden, width), BF16),
            vmem((tp, slots, width), BF16),
            vmem((tp - 1, slots, width), BF16),
            vmem((slots * SUB, LANE), BF16),
            vmem((slots * SUB, LANE), BF16),
            dma(7), dma(tp - 1), dma(tp - 1), dma(ep), dma(ep), dma(tp - 1, 8), dma(tp - 1, 8),
            dma(tp - 1, 2), dma(tp - 1, 2), dma(ep), dma(ep), dma(tp - 1), dma(tp - 1),
            dma(2, 2, hops), dma(2, 2, hops), dma(2, 2, hops), dma(2, 2, hops),
        ],
        compiler_params=pltpu.CompilerParams(
            collective_id=0, has_side_effects=True, vmem_limit_bytes=63 * 1024 * 1024
        ),
    )(
        mixer_input, mixer_gain[None], query_weight, key_weight, value_weight, out_weight,
        post_gain[None], forget_cumsum, expert_input, expert_gain[None], routes.T, route_weight.T,
        expert_gate, expert_upward, expert_down,
    )
    return pl.pallas_call(
        hand_over,
        name="hand_over",
        out_shape=[jax.ShapeDtypeStruct(r.shape, r.dtype) for r in results],
        in_specs=[VM, VM],
        out_specs=[VM, VM],
    )(*results)


def solution(mesh):
    rows = P(("grp", "ep", "tp"), None)
    in_specs = (
        rows, P("tp", "grp"), P(), P(None, "tp"), P(None, "tp"), P(None, "tp"), P("tp", None), P(),
        rows, P(), rows, rows, P("ep", None, "tp"), P("ep", None, "tp"), P("ep", "tp", None),
    )
    return jax.shard_map(
        on_device, mesh=mesh, in_specs=in_specs, out_specs=(rows, rows), check_vma=False
    )
```

```python
import functools

import jax
import jax.numpy as jnp
from jax import lax
from jax.experimental import pallas as pl
from jax.experimental.pallas import tpu as pltpu
from jax.sharding import PartitionSpec as P

EPS = 1e-06
MASKED = -1e30
LOG2E = 1.4426950408889634
MESH = pl.DeviceIdType.MESH
SUB, LANE = 16, 128
TOP = 2
SERVE = ((0, 0), (1, 5))
REDUCE = ((0, 9), (1, 13))
GIVE = ((0, 32, 13),)
BF16, F32 = jnp.bfloat16, jnp.float32
ANY = pl.BlockSpec(memory_space=pl.ANY)
VM = pl.BlockSpec(memory_space=pltpu.VMEM)


def normalize(row_block, gain):
    values = row_block.astype(F32)
    inverse = lax.rsqrt(jnp.mean(values * values, axis=-1, keepdims=True) + EPS)
    return values * inverse * gain


def dot(a, b):
    return jnp.dot(a, b, preferred_element_type=F32)


def swap_matrix():
    n = SUB * SUB
    i = lax.broadcasted_iota(jnp.int32, (n, n), 0)
    k = lax.broadcasted_iota(jnp.int32, (n, n), 1)
    hit = ((i // SUB) == (k % SUB)) & ((i % SUB) == (k // SUB))
    return jnp.where(hit, 1.0, 0.0).astype(BF16)


def to_wire(swap, rows):
    count = rows.shape[0] // SUB
    halves = [
        jnp.concatenate(
            [rows[SUB * a : SUB * (a + 1), LANE * s : LANE * (s + 1)] for s in range(SUB)], axis=0
        )
        for a in range(count)
    ]
    out = dot(swap, jnp.concatenate(halves, axis=1)).astype(BF16)
    return jnp.concatenate([out[:, LANE * a : LANE * (a + 1)] for a in range(count)], axis=0)


def from_wire(swap, tiles):
    n = SUB * SUB
    count = tiles.shape[0] // n
    out = dot(swap, jnp.concatenate([tiles[n * a : n * (a + 1)] for a in range(count)], axis=1))
    out = out.astype(BF16)
    halves = [
        jnp.concatenate(
            [out[SUB * s : SUB * (s + 1), LANE * a : LANE * (a + 1)] for s in range(SUB)], axis=1
        )
        for a in range(count)
    ]
    return jnp.concatenate(halves, axis=0)


def upright(ref):
    top, rows = ref.shape
    return jnp.transpose(
        jnp.concatenate([ref[...].astype(F32), jnp.zeros((8 - top, rows), F32)], axis=0)
    )


def slot_columns(routes):
    rows, top = routes.shape[0], TOP
    experts = lax.broadcasted_iota(jnp.int32, (rows, LANE), 1).astype(F32)
    earlier = lax.broadcasted_iota(jnp.int32, (rows, rows), 1) < lax.broadcasted_iota(
        jnp.int32, (rows, rows), 0
    )
    earlier = jnp.where(earlier, 1.0, 0.0).astype(BF16)
    taken = jnp.zeros((1, LANE), F32)
    columns = []
    for k in range(top):
        member = jnp.where(experts == routes[:, k : k + 1], 1.0, 0.0)
        before = dot(earlier, member.astype(BF16)) + taken
        rank = jnp.sum(before * member, axis=1, keepdims=True)
        columns.append((routes[:, k : k + 1], rank))
        taken = taken + jnp.sum(member, axis=0, keepdims=True)
    return columns


def chooser(column, width):
    ids = lax.broadcasted_iota(jnp.int32, (column.shape[0], width), 1).astype(F32)
    return jnp.where(ids == column, 1.0, 0.0)


def greet(axes):
    barrier = pltpu.get_barrier_semaphore()
    total = 0
    for axis in axes:
        n = lax.axis_size(axis)
        me = lax.axis_index(axis)

        @pl.loop(1, n)
        def _(s):
            pl.semaphore_signal(
                barrier, inc=1, device_id={axis: lax.rem(me + s, n)}, device_id_type=MESH
            )

        total += n - 1
    return lambda: pl.semaphore_wait(barrier, total)


def remote(src, dst, send_sem, recv_sem, **device):
    return pltpu.make_async_remote_copy(
        src_ref=src, dst_ref=dst, send_sem=send_sem, recv_sem=recv_sem,
        device_id=device, device_id_type=MESH,
    )


def aligned(start, size):
    return pl.ds(pl.multiple_of(start, size), size)


def attend_block(queries, pair, bias, running_max, running_sum, running_acc, masked):
    heads, span, head_dim = running_acc.shape
    scale = head_dim ** (-0.5) * LOG2E
    for h in range(heads):
        cols = slice(h * head_dim, (h + 1) * head_dim)
        scores = lax.dot_general(
            queries[:, cols], pair[0, :, cols], (((1,), (1,)), ((), ())), preferred_element_type=F32
        )
        scores = scores * scale + bias[h : h + 1, :]
        if masked:
            seen = lax.broadcasted_iota(jnp.int32, (span, span), 1) <= (
                lax.broadcasted_iota(jnp.int32, (span, span), 0)
            )
            scores = jnp.where(seen, scores, MASKED)
        old = running_max[h]
        new = jnp.maximum(old, jnp.max(scores, axis=1, keepdims=True))
        weights = jnp.exp2(scores - jnp.tile(new, (1, span // LANE)))
        rescale = jnp.exp2(old - new)
        partial = weights[:, :LANE]
        for i in range(1, span // LANE):
            partial = partial + weights[:, i * LANE : (i + 1) * LANE]
        running_sum[h] = running_sum[h] * rescale + partial
        running_acc[h] = running_acc[h] * rescale + dot(weights.astype(BF16), pair[1, :, cols])
        running_max[h] = new


def expert_block(swap, stack, gate, up, down, sums, start, piece):
    tiles = piece * SUB
    half_tiles = 256 * (piece // SUB // 2)
    got = [
        from_wire(swap, stack[pl.ds(pl.multiple_of(start * SUB + at, 256), size), :])
        for at, size in ((0, half_tiles), (half_tiles, tiles - half_tiles))
    ]
    batch = jnp.concatenate(got, axis=0)
    gate_proj = dot(batch, gate[0])
    hidden = (gate_proj / (1.0 + jnp.exp(-gate_proj)) * dot(batch, up[0])).astype(BF16)
    sums[aligned(start, piece), :] = dot(hidden, down[0]).astype(BF16)


def kernel(
    capacity,
    x_ref, gain_ref, wq_ref, wk_ref, wv_ref, wo_ref, post_ref, forget_ref,
    y_ref, ygain_ref, routes_ref, rweight_ref, gate_ref, up_ref, down_ref,
    mix_ref, out_ref,
    normed, qkv_w, queries, keys, out_w, running_max, running_sum, running_acc, attended, parts, mix_theirs,
    natural, send, stack, gate, up, down, sums, theirs, back, returned, picks, combined,
    w_sem, ns_sem, nr_sem, zs_sem, zr_sem, gs_sem, gr_sem, ps_sem, pr_sem, bs_sem, br_sem, ms_sem, mr_sem,
    rs_sem, rr_sem, cs_sem, cr_sem,
):
    rows, width = x_ref.shape
    head_width = wq_ref.shape[1]
    heads = forget_ref.shape[0]
    head_dim = head_width // heads
    tp, t = lax.axis_size("tp"), lax.axis_index("tp")
    ep, e = lax.axis_size("ep"), lax.axis_index("ep")
    chips, chip, core = ep // 2, e // 2, lax.rem(e, 2)
    span = rows * tp
    slots = natural.shape[0]
    block = capacity * SUB
    pieces = 2
    piece = slots // pieces
    groups = 8
    group = ep // groups
    peers = (1, tp - 1) + tuple(range(2, tp - 1))

    loads = [
        pltpu.make_async_copy(src, dst, w_sem.at[i])
        for i, (src, dst) in enumerate(
            (
                (wq_ref, qkv_w.at[0]), (wk_ref, qkv_w.at[1]), (wv_ref, qkv_w.at[2]),
                (gate_ref, gate), (up_ref, up), (down_ref, down), (wo_ref, out_w),
            )
        )
    ]
    for load in loads:
        load.start()
    met = greet(("ep", "tp"))

    columns = [expert * capacity + rank for expert, rank in slot_columns(upright(routes_ref))]
    padded = -(-slots // LANE) * LANE
    choose = sum(chooser(c, padded) for c in columns)
    expert_rows = normalize(y_ref[...], ygain_ref[...]).astype(BF16)
    natural[...] = dot(jnp.transpose(choose)[:slots].astype(BF16), expert_rows).astype(BF16)
    swap = swap_matrix()
    for c in range(slots // 32):
        send[pl.ds(c * 512, 512), :] = to_wire(swap, natural[pl.ds(c * 32, 32), :])
    met()

    def offset(p):
        return lax.rem(p, 2) * ((p + 1) // 2) + (1 - lax.rem(p, 2)) * (ep - p // 2)

    def dispatch(p):
        to = lax.rem(e + offset(p), ep)
        return remote(
            send.at[aligned(to * block, block)], stack.at[0, aligned(p * block, block)],
            zs_sem.at[p], zr_sem.at[p], ep=to,
        )

    @pl.loop(1, ep)
    def _(p):
        dispatch(p).start()

    stack[0, :block, :] = send[aligned(e * block, block), :]

    own = aligned(t * rows, rows)
    normed[own, :] = normalize(x_ref[...], gain_ref[...]).astype(BF16)

    def spread(j):
        return remote(
            normed.at[own], normed.at[own], ns_sem.at[j - 1], nr_sem.at[j - 1], tp=lax.rem(t + j, tp)
        )

    for j in peers:
        spread(j).start()
    running_max[...] = jnp.full_like(running_max, MASKED)
    running_sum[...] = jnp.zeros_like(running_sum)
    running_acc[...] = jnp.zeros_like(running_acc)
    for load in loads:
        load.wait()
    for j in (0,) + peers:
        if j:
            spread(j).wait_recv()
        part = aligned(lax.rem(t + tp - j, tp) * rows, rows)
        block_rows = normed[part, :]
        queries[part, :] = dot(block_rows, qkv_w[0]).astype(BF16)
        for half in range(2):
            keys[e, half, part, :] = dot(block_rows, qkv_w[1 + half]).astype(BF16)

    def source(way, h):
        return lax.rem(chip + (chips - h if way == 0 else h), chips)

    def hop(way, half, h):
        at = 2 * source(way, h - 1) + core
        to = lax.rem(e + (2 if way == 0 else ep - 2), ep)
        return remote(
            keys.at[at, half], keys.at[at, half], rs_sem.at[way, half, h], rr_sem.at[way, half, h], ep=to
        )

    def share(way, half, h):
        at = 2 * source(way, h) + core
        return remote(
            keys.at[at, half], keys.at[at, half], cs_sem.at[way, half, h], cr_sem.at[way, half, h],
            ep=e + 1 - 2 * core,
        )

    def farthest(way, half):
        return chips // 2 if way == half else chips // 2 - 1

    def comes(way, half, h):
        near = h <= farthest(way, half)
        return near & (chip >= h if way == 0 else lax.rem(chip + h, chips) < chips // 2)

    def needed(way, half, h):
        return (h <= farthest(way, half)) & (chip >= h if way == 0 else chip + h >= chips)

    def goes(way, half, h):
        near = h <= farthest(way, half)
        if way == 0:
            return near & (chip >= h - 1) & (chip + 1 < chips)
        return near & (lax.rem(chip + h - 1, chips) < chips // 2)

    WAYS = [(way, half) for half in range(2) for way in range(2)]
    for way, half in WAYS:
        @pl.when(goes(way, half, 1))
        def _():
            hop(way, half, 1).start()

    for half in range(2):
        share(0, half, 0).start()

    def forth(j, g):
        size = group * block
        return remote(
            stack.at[0, aligned(g * size, size)], stack.at[j, aligned(g * size, size)],
            gs_sem.at[j - 1, g], gr_sem.at[j - 1, g], tp=lax.rem(t + j, tp),
        )

    def back_to(j, p):
        return remote(
            sums.at[j, aligned(p * piece, piece)], theirs.at[j - 1, aligned(p * piece, piece)],
            ps_sem.at[j - 1, p], pr_sem.at[j - 1, p], tp=lax.rem(t + tp - j, tp),
        )

    def expert(j, p):
        expert_block(swap, stack.at[j], gate, up, down, sums.at[j], p * piece, piece)

    @pl.loop(0, groups)
    def _(g):
        @pl.loop(0, group)
        def _(i):
            @pl.when(g * group + i > 0)
            def _():
                dispatch(g * group + i).wait_recv()

        for j in peers:
            forth(j, g).start()

    @pl.loop(0, pieces)
    def _(p):
        expert(0, p)

    def serve(i, p):
        j = i + (i // 2) * (1 - 2 * (i % 2))

        @pl.loop(0, groups // pieces)
        def _(g):
            forth(j, p * (groups // pieces) + g).wait_recv()

        expert(j, p)
        back_to(j, p).start()

    def give_back(p):
        from_here = lax.rem(e + ep - offset(p), ep)
        return remote(
            back.at[aligned(p * block, block)], returned.at[aligned(p * block, block)],
            bs_sem.at[p], br_sem.at[p], ep=from_here,
        )

    def reduce(p):
        for j in peers:
            back_to(j, p).wait_recv()

        @pl.loop(0, piece // SUB)
        def _(i):
            here = pl.ds(pl.multiple_of(p * piece + SUB * i, SUB), SUB)
            total = sums[0, here, :].astype(F32)
            for j in range(1, tp):
                total = total + theirs[j - 1, here, :].astype(F32)
            back[pl.ds(pl.multiple_of((p * piece + SUB * i) * SUB, 256), 256), :] = to_wire(
                swap, total.astype(BF16)
            )

    def give(low, high):
        @pl.loop(max(low, 1), high)
        def _(p):
            give_back(p).start()

    base = forget_ref[:, aligned(e * span, span)][:, :1]

    def attend(j, masked):
        bias = (base - forget_ref[:, aligned(j * span, span)]) * LOG2E
        attend_block(
            queries, keys.at[j], bias, running_max, running_sum, running_acc, masked
        )

    attend(e, True)
    last = chips // 2

    def pump(half, h):
        for way in range(2):
            @pl.when(comes(way, half, h))
            def _():
                hop(way, half, h).wait_recv()

                @pl.when(goes(way, half, h + 1))
                def _():
                    hop(way, half, h + 1).start()

                @pl.when(needed(way, half, h))
                def _():
                    share(way, half, h).start()

    @pl.loop(0, 2 * last + 2)
    def _(u):
        h, half = u // 2 + 1, lax.rem(u, 2)
        g = h - 1
        for which in range(2):
            @pl.when(half == which)
            def _():
                pump(which, h)

        @pl.when(half == 0)
        def _():
            for way, what in WAYS:
                @pl.when(needed(way, what, g))
                def _():
                    share(way, what, g).wait_recv()

        @pl.loop(0, 2)
        def _(parity):
            away = (g > 0) & (
                ((half == 0) & (chip >= g)) | ((half == 1) & (chip + g >= chips) & (g < last))
            )
            home = (u == 0) & (parity == 0) & (core == 1)

            @pl.when(away | home)
            def _():
                attend(2 * (chip - g + half * (2 * g - chips)) + parity, False)

        for p, first in SERVE:
            for i in range(1, tp):
                @pl.when(u == first + i - 1)
                def _():
                    serve(i, p)

        for p, at in REDUCE:
            @pl.when(u == at)
            def _():
                reduce(p)

        for low, high, at in GIVE:
            @pl.when(u == at)
            def _():
                give(low, high)

    for h in range(heads):
        total = jnp.sum(running_sum[h], axis=1, keepdims=True)
        attended[:, h * head_dim : (h + 1) * head_dim] = (running_acc[h] / total).astype(BF16)

    def mix_to(j):
        return remote(
            parts.at[j], mix_theirs.at[j - 1], ms_sem.at[j - 1], mr_sem.at[j - 1], tp=lax.rem(t + j, tp)
        )

    for j in tuple(range(2, tp - 1)) + (1, tp - 1, 0):
        here = aligned(lax.rem(t + j, tp) * rows, rows)
        parts[j] = dot(attended[here, :], out_w[...]).astype(BF16)
        if j:
            mix_to(j).start()

    returned[:block, :] = back[:block, :]
    half_slots = slots // 2
    rweight = upright(rweight_ref)
    places = []
    for chosen_expert, rank in slot_columns(upright(routes_ref)):
        ahead = chosen_expert - e.astype(F32)
        ahead = jnp.where(ahead < 0, ahead + ep, ahead)
        place = jnp.where(ahead > ep // 2, 2 * (ep - ahead), jnp.maximum(2 * ahead - 1, 0))
        places.append(place * capacity + rank)
    for stage in range(2):
        picks[stage] = jnp.concatenate(
            [chooser(place - stage * half_slots, half_slots) for place in places], axis=0
        ).astype(BF16)

    total = parts[0].astype(F32)
    for j in range(1, tp):
        mix_to(j).wait_recv()
        total = total + mix_theirs[j - 1].astype(F32)
    mix_ref[...] = normalize(total, post_ref[...]).astype(BF16)

    for stage in range(2):
        @pl.loop(max(stage * (ep // 2), 1), (stage + 1) * (ep // 2))
        def _(p):
            give_back(p).wait_recv()

        here = stage * half_slots
        for at in range(0, half_slots, 48):
            natural[pl.ds(here + at, 48), :] = from_wire(
                swap, returned[pl.ds((here + at) * SUB, 48 * SUB), :]
            )
        both = dot(picks[stage], natural[pl.ds(here, half_slots), :])
        result = rweight[:, :1] * both[:rows] + rweight[:, 1:2] * both[rows:]
        if stage == 0:
            combined[...] = result
        else:
            out_ref[...] = (combined[...] + result).astype(BF16)

    for j in range(1, tp):
        spread(j).wait_send()
        mix_to(j).wait_send()
        for p in range(pieces):
            back_to(j, p).wait_send()

        @pl.loop(0, groups)
        def _(g):
            forth(j, g).wait_send()

    @pl.loop(1, ep)
    def _(p):
        dispatch(p).wait_send()
        give_back(p).wait_send()

    for half in range(2):
        share(0, half, 0).wait_send()

    @pl.loop(1, last + 1)
    def _(h):
        for way, half in WAYS:
            @pl.when(goes(way, half, h))
            def _():
                hop(way, half, h).wait_send()

            @pl.when(needed(way, half, h))
            def _():
                share(way, half, h).wait_send()


def hand_over(mix_ref, out_ref, mix_result, out_result):
    mix_result[...] = mix_ref[...]
    out_result[...] = out_ref[...]


def dma(*shape):
    return pltpu.SemaphoreType.DMA(shape)


def on_device(
    mixer_input, forget_cumsum, mixer_gain, query_weight, key_weight, value_weight, out_weight,
    post_gain, expert_input, expert_gain, routes, route_weight, expert_gate, expert_upward, expert_down,
):
    ep, tp = lax.axis_size("ep"), lax.axis_size("tp")
    rows, width = mixer_input.shape
    heads = forget_cumsum.shape[0]
    head_width = query_weight.shape[1]
    head_dim = head_width // heads
    span = rows * tp
    moe_rows, top = routes.shape
    experts = ep * expert_gate.shape[0]
    capacity = (moe_rows * top * 9 + 8 * experts - 1) // (8 * experts)
    slots = experts * capacity
    hidden = expert_gate.shape[2]
    vmem = pltpu.VMEM
    hops = ep // 4 + 3

    results = pl.pallas_call(
        functools.partial(kernel, capacity),
        name="block",
        out_shape=(
            jax.ShapeDtypeStruct((rows, width), BF16),
            jax.ShapeDtypeStruct((moe_rows, width), BF16),
        ),
        in_specs=[VM, VM, ANY, ANY, ANY, ANY, VM, VM, VM, VM, VM, VM, ANY, ANY, ANY],
        out_specs=(VM, VM),
        scratch_shapes=[
            vmem((span, width), BF16),
            vmem((3, width, head_width), BF16),
            vmem((span, head_width), BF16),
            vmem((ep, 2, span, head_width), BF16),
            vmem((head_width, width), BF16),
            vmem((heads, span, LANE), F32),
            vmem((heads, span, LANE), F32),
            vmem((heads, span, head_dim), F32),
            vmem((span, head_width), BF16),
            vmem((tp, rows, width), BF16),
            vmem((tp - 1, rows, width), BF16),
            vmem((slots, width), BF16),
            vmem((slots * SUB, LANE), BF16),
            vmem((tp, slots * SUB, LANE), BF16),
            vmem((1, width, hidden), BF16),
            vmem((1, width, hidden), BF16),
            vmem((1, hidden, width), BF16),
            vmem((tp, slots, width), BF16),
            vmem((tp - 1, slots, width), BF16),
            vmem((slots * SUB, LANE), BF16),
            vmem((slots * SUB, LANE), BF16),
            vmem((2, top * moe_rows, slots // 2), BF16),
            vmem((moe_rows, width), F32),
            dma(7), dma(tp - 1), dma(tp - 1), dma(ep), dma(ep), dma(tp - 1, 8), dma(tp - 1, 8),
            dma(tp - 1, 2), dma(tp - 1, 2), dma(ep), dma(ep), dma(tp - 1), dma(tp - 1),
            dma(2, 2, hops), dma(2, 2, hops), dma(2, 2, hops), dma(2, 2, hops),
        ],
        compiler_params=pltpu.CompilerParams(
            collective_id=0, has_side_effects=True, vmem_limit_bytes=63 * 1024 * 1024
        ),
    )(
        mixer_input, mixer_gain[None], query_weight, key_weight, value_weight, out_weight,
        post_gain[None], forget_cumsum, expert_input, expert_gain[None], routes.T, route_weight.T,
        expert_gate, expert_upward, expert_down,
    )
    return pl.pallas_call(
        hand_over,
        name="hand_over",
        out_shape=[jax.ShapeDtypeStruct(r.shape, r.dtype) for r in results],
        in_specs=[VM, VM],
        out_specs=[VM, VM],
    )(*results)


def solution(mesh):
    rows = P(("grp", "ep", "tp"), None)
    in_specs = (
        rows, P("tp", "grp"), P(), P(None, "tp"), P(None, "tp"), P(None, "tp"), P("tp", None), P(),
        rows, P(), rows, rows, P("ep", None, "tp"), P("ep", None, "tp"), P("ep", "tp", None),
    )
    return jax.shard_map(
        on_device, mesh=mesh, in_specs=in_specs, out_specs=(rows, rows), check_vma=False
    )
```

```python
import functools

import jax
import jax.numpy as jnp
from jax import lax
from jax.experimental import pallas as pl
from jax.experimental.pallas import tpu as pltpu
from jax.sharding import PartitionSpec as P

EPS = 1e-06
MASKED = -1e30
LOG2E = 1.4426950408889634
MESH = pl.DeviceIdType.MESH
SUB, LANE = 16, 128
TOP = 2
SERVE = ((0, 0), (1, 5))
REDUCE = ((0, 9), (1, 13))
NEAR, LOW = 13, 6
BF16, F32 = jnp.bfloat16, jnp.float32
ANY = pl.BlockSpec(memory_space=pl.ANY)
VM = pl.BlockSpec(memory_space=pltpu.VMEM)


def normalize(row_block, gain):
    values = row_block.astype(F32)
    inverse = lax.rsqrt(jnp.mean(values * values, axis=-1, keepdims=True) + EPS)
    return values * inverse * gain


def dot(a, b):
    return jnp.dot(a, b, preferred_element_type=F32)


def swap_matrix():
    n = SUB * SUB
    i = lax.broadcasted_iota(jnp.int32, (n, n), 0)
    k = lax.broadcasted_iota(jnp.int32, (n, n), 1)
    hit = ((i // SUB) == (k % SUB)) & ((i % SUB) == (k // SUB))
    return jnp.where(hit, 1.0, 0.0).astype(BF16)


def to_wire(swap, rows):
    count = rows.shape[0] // SUB
    halves = [
        jnp.concatenate(
            [rows[SUB * a : SUB * (a + 1), LANE * s : LANE * (s + 1)] for s in range(SUB)], axis=0
        )
        for a in range(count)
    ]
    out = dot(swap, jnp.concatenate(halves, axis=1)).astype(BF16)
    return jnp.concatenate([out[:, LANE * a : LANE * (a + 1)] for a in range(count)], axis=0)


def from_wire(swap, tiles):
    n = SUB * SUB
    count = tiles.shape[0] // n
    out = dot(swap, jnp.concatenate([tiles[n * a : n * (a + 1)] for a in range(count)], axis=1))
    out = out.astype(BF16)
    halves = [
        jnp.concatenate(
            [out[SUB * s : SUB * (s + 1), LANE * a : LANE * (a + 1)] for s in range(SUB)], axis=1
        )
        for a in range(count)
    ]
    return jnp.concatenate(halves, axis=0)


def upright(ref):
    top, rows = ref.shape
    return jnp.transpose(
        jnp.concatenate([ref[...].astype(F32), jnp.zeros((8 - top, rows), F32)], axis=0)
    )


def slot_columns(routes):
    rows, top = routes.shape[0], TOP
    experts = lax.broadcasted_iota(jnp.int32, (rows, LANE), 1).astype(F32)
    earlier = lax.broadcasted_iota(jnp.int32, (rows, rows), 1) < lax.broadcasted_iota(
        jnp.int32, (rows, rows), 0
    )
    earlier = jnp.where(earlier, 1.0, 0.0).astype(BF16)
    taken = jnp.zeros((1, LANE), F32)
    columns = []
    for k in range(top):
        member = jnp.where(experts == routes[:, k : k + 1], 1.0, 0.0)
        before = dot(earlier, member.astype(BF16)) + taken
        rank = jnp.sum(before * member, axis=1, keepdims=True)
        columns.append((routes[:, k : k + 1], rank))
        taken = taken + jnp.sum(member, axis=0, keepdims=True)
    return columns


def chooser(column, width):
    ids = lax.broadcasted_iota(jnp.int32, (column.shape[0], width), 1).astype(F32)
    return jnp.where(ids == column, 1.0, 0.0)


def greet(axes):
    barrier = pltpu.get_barrier_semaphore()
    total = 0
    for axis in axes:
        n = lax.axis_size(axis)
        me = lax.axis_index(axis)

        @pl.loop(1, n)
        def _(s):
            pl.semaphore_signal(
                barrier, inc=1, device_id={axis: lax.rem(me + s, n)}, device_id_type=MESH
            )

        total += n - 1
    return lambda: pl.semaphore_wait(barrier, total)


def remote(src, dst, send_sem, recv_sem, **device):
    return pltpu.make_async_remote_copy(
        src_ref=src, dst_ref=dst, send_sem=send_sem, recv_sem=recv_sem,
        device_id=device, device_id_type=MESH,
    )


def aligned(start, size):
    return pl.ds(pl.multiple_of(start, size), size)


def attend_block(queries, pair, bias, running_max, running_sum, running_acc, masked):
    heads, span, head_dim = running_acc.shape
    scale = head_dim ** (-0.5) * LOG2E
    for h in range(heads):
        cols = slice(h * head_dim, (h + 1) * head_dim)
        scores = lax.dot_general(
            queries[:, cols], pair[0, :, cols], (((1,), (1,)), ((), ())), preferred_element_type=F32
        )
        scores = scores * scale + bias[h : h + 1, :]
        if masked:
            seen = lax.broadcasted_iota(jnp.int32, (span, span), 1) <= (
                lax.broadcasted_iota(jnp.int32, (span, span), 0)
            )
            scores = jnp.where(seen, scores, MASKED)
        old = running_max[h]
        new = jnp.maximum(old, jnp.max(scores, axis=1, keepdims=True))
        weights = jnp.exp2(scores - jnp.tile(new, (1, span // LANE)))
        rescale = jnp.exp2(old - new)
        partial = weights[:, :LANE]
        for i in range(1, span // LANE):
            partial = partial + weights[:, i * LANE : (i + 1) * LANE]
        running_sum[h] = running_sum[h] * rescale + partial
        running_acc[h] = running_acc[h] * rescale + dot(weights.astype(BF16), pair[1, :, cols])
        running_max[h] = new


def expert_block(swap, stack, gate, up, down, sums, start, piece):
    tiles = piece * SUB
    half_tiles = 256 * (piece // SUB // 2)
    got = [
        from_wire(swap, stack[pl.ds(pl.multiple_of(start * SUB + at, 256), size), :])
        for at, size in ((0, half_tiles), (half_tiles, tiles - half_tiles))
    ]
    batch = jnp.concatenate(got, axis=0)
    gate_proj = dot(batch, gate[0])
    hidden = (gate_proj / (1.0 + jnp.exp(-gate_proj)) * dot(batch, up[0])).astype(BF16)
    sums[aligned(start, piece), :] = dot(hidden, down[0]).astype(BF16)


def kernel(
    capacity,
    x_ref, gain_ref, wq_ref, wk_ref, wv_ref, wo_ref, post_ref, forget_ref,
    y_ref, ygain_ref, routes_ref, rweight_ref, gate_ref, up_ref, down_ref,
    mix_ref, out_ref,
    normed, qkv_w, queries, keys, out_w, running_max, running_sum, running_acc, attended, parts, mix_theirs,
    natural, send, stack, gate, up, down, sums, theirs, back, returned, picks, combined,
    w_sem, ns_sem, nr_sem, zs_sem, zr_sem, gs_sem, gr_sem, ps_sem, pr_sem, bs_sem, br_sem, ms_sem, mr_sem,
    rs_sem, rr_sem, cs_sem, cr_sem,
):
    rows, width = x_ref.shape
    head_width = wq_ref.shape[1]
    heads = forget_ref.shape[0]
    head_dim = head_width // heads
    tp, t = lax.axis_size("tp"), lax.axis_index("tp")
    ep, e = lax.axis_size("ep"), lax.axis_index("ep")
    chips, chip, core = ep // 2, e // 2, lax.rem(e, 2)
    span = rows * tp
    slots = natural.shape[0]
    block = capacity * SUB
    pieces = 2
    piece = slots // pieces
    groups = 8
    group = ep // groups
    peers = (1, tp - 1) + tuple(range(2, tp - 1))

    loads = [
        pltpu.make_async_copy(src, dst, w_sem.at[i])
        for i, (src, dst) in enumerate(
            (
                (wq_ref, qkv_w.at[0]), (wk_ref, qkv_w.at[1]), (wv_ref, qkv_w.at[2]),
                (gate_ref, gate), (up_ref, up), (down_ref, down), (wo_ref, out_w),
            )
        )
    ]
    for load in loads:
        load.start()
    met = greet(("ep", "tp"))

    columns = [expert * capacity + rank for expert, rank in slot_columns(upright(routes_ref))]
    padded = -(-slots // LANE) * LANE
    choose = sum(chooser(c, padded) for c in columns)
    expert_rows = normalize(y_ref[...], ygain_ref[...]).astype(BF16)
    natural[...] = dot(jnp.transpose(choose)[:slots].astype(BF16), expert_rows).astype(BF16)
    swap = swap_matrix()
    for c in range(slots // 32):
        send[pl.ds(c * 512, 512), :] = to_wire(swap, natural[pl.ds(c * 32, 32), :])
    met()

    def offset(p):
        return lax.rem(p, 2) * ((p + 1) // 2) + (1 - lax.rem(p, 2)) * (ep - p // 2)

    def dispatch(p):
        to = lax.rem(e + offset(p), ep)
        return remote(
            send.at[aligned(to * block, block)], stack.at[0, aligned(p * block, block)],
            zs_sem.at[p], zr_sem.at[p], ep=to,
        )

    @pl.loop(1, ep)
    def _(p):
        dispatch(p).start()

    stack[0, :block, :] = send[aligned(e * block, block), :]

    own = aligned(t * rows, rows)
    normed[own, :] = normalize(x_ref[...], gain_ref[...]).astype(BF16)

    def spread(j):
        return remote(
            normed.at[own], normed.at[own], ns_sem.at[j - 1], nr_sem.at[j - 1], tp=lax.rem(t + j, tp)
        )

    for j in peers:
        spread(j).start()
    running_max[...] = jnp.full_like(running_max, MASKED)
    running_sum[...] = jnp.zeros_like(running_sum)
    running_acc[...] = jnp.zeros_like(running_acc)
    for load in loads:
        load.wait()
    for j in (0,) + peers:
        if j:
            spread(j).wait_recv()
        part = aligned(lax.rem(t + tp - j, tp) * rows, rows)
        block_rows = normed[part, :]
        queries[part, :] = dot(block_rows, qkv_w[0]).astype(BF16)
        for half in range(2):
            keys[e, half, part, :] = dot(block_rows, qkv_w[1 + half]).astype(BF16)

    def source(way, h):
        return lax.rem(chip + (chips - h if way == 0 else h), chips)

    def hop(way, half, h):
        at = 2 * source(way, h - 1) + core
        to = lax.rem(e + (2 if way == 0 else ep - 2), ep)
        return remote(
            keys.at[at, half], keys.at[at, half], rs_sem.at[way, half, h], rr_sem.at[way, half, h], ep=to
        )

    def share(way, half, h):
        at = 2 * source(way, h) + core
        return remote(
            keys.at[at, half], keys.at[at, half], cs_sem.at[way, half, h], cr_sem.at[way, half, h],
            ep=e + 1 - 2 * core,
        )

    def farthest(way, half):
        return chips // 2 if way == half else chips // 2 - 1

    def comes(way, half, h):
        near = h <= farthest(way, half)
        return near & (chip >= h if way == 0 else lax.rem(chip + h, chips) < chips // 2)

    def needed(way, half, h):
        return (h <= farthest(way, half)) & (chip >= h if way == 0 else chip + h >= chips)

    def goes(way, half, h):
        near = h <= farthest(way, half)
        if way == 0:
            return near & (chip >= h - 1) & (chip + 1 < chips)
        return near & (lax.rem(chip + h - 1, chips) < chips // 2)

    WAYS = [(way, half) for half in range(2) for way in range(2)]
    for way, half in WAYS:
        @pl.when(goes(way, half, 1))
        def _():
            hop(way, half, 1).start()

    for half in range(2):
        share(0, half, 0).start()

    def forth(j, g):
        size = group * block
        return remote(
            stack.at[0, aligned(g * size, size)], stack.at[j, aligned(g * size, size)],
            gs_sem.at[j - 1, g], gr_sem.at[j - 1, g], tp=lax.rem(t + j, tp),
        )

    def back_to(j, p):
        return remote(
            sums.at[j, aligned(p * piece, piece)], theirs.at[j - 1, aligned(p * piece, piece)],
            ps_sem.at[j - 1, p], pr_sem.at[j - 1, p], tp=lax.rem(t + tp - j, tp),
        )

    def expert(j, p):
        expert_block(swap, stack.at[j], gate, up, down, sums.at[j], p * piece, piece)

    @pl.loop(0, groups)
    def _(g):
        @pl.loop(0, group)
        def _(i):
            @pl.when(g * group + i > 0)
            def _():
                dispatch(g * group + i).wait_recv()

        for j in peers:
            forth(j, g).start()

    @pl.loop(0, pieces)
    def _(p):
        expert(0, p)

    def serve(i, p):
        j = i + (i // 2) * (1 - 2 * (i % 2))

        @pl.loop(0, groups // pieces)
        def _(g):
            forth(j, p * (groups // pieces) + g).wait_recv()

        expert(j, p)
        back_to(j, p).start()

    def give_back(p):
        from_here = lax.rem(e + ep - offset(p), ep)
        return remote(
            back.at[aligned(p * block, block)], returned.at[aligned(p * block, block)],
            bs_sem.at[p], br_sem.at[p], ep=from_here,
        )

    def reduce(p):
        for j in peers:
            back_to(j, p).wait_recv()

        @pl.loop(0, piece // SUB)
        def _(i):
            here = pl.ds(pl.multiple_of(p * piece + SUB * i, SUB), SUB)
            total = sums[0, here, :].astype(F32)
            for j in range(1, tp):
                total = total + theirs[j - 1, here, :].astype(F32)
            back[pl.ds(pl.multiple_of((p * piece + SUB * i) * SUB, 256), 256), :] = to_wire(
                swap, total.astype(BF16)
            )

    def give():
        @pl.loop(1, NEAR)
        def _(p):
            give_back(p).start()

        for low in (True, False):
            @pl.loop(NEAR, ep)
            def _(p):
                to_low = lax.rem(e + ep - offset(p), ep) < LOW

                @pl.when(to_low if low else jnp.logical_not(to_low))
                def _():
                    give_back(p).start()

    base = forget_ref[:, aligned(e * span, span)][:, :1]

    def attend(j, masked):
        bias = (base - forget_ref[:, aligned(j * span, span)]) * LOG2E
        attend_block(
            queries, keys.at[j], bias, running_max, running_sum, running_acc, masked
        )

    attend(e, True)
    last = chips // 2

    def pump(half, h):
        for way in range(2):
            @pl.when(comes(way, half, h))
            def _():
                hop(way, half, h).wait_recv()

                @pl.when(goes(way, half, h + 1))
                def _():
                    hop(way, half, h + 1).start()

                @pl.when(needed(way, half, h))
                def _():
                    share(way, half, h).start()

    @pl.loop(0, 2 * last + 2)
    def _(u):
        h, half = u // 2 + 1, lax.rem(u, 2)
        g = h - 1
        for which in range(2):
            @pl.when(half == which)
            def _():
                pump(which, h)

        @pl.when(half == 0)
        def _():
            for way, what in WAYS:
                @pl.when(needed(way, what, g))
                def _():
                    share(way, what, g).wait_recv()

        @pl.loop(0, 2)
        def _(parity):
            away = (g > 0) & (
                ((half == 0) & (chip >= g)) | ((half == 1) & (chip + g >= chips) & (g < last))
            )
            home = (u == 0) & (parity == 0) & (core == 1)

            @pl.when(away | home)
            def _():
                attend(2 * (chip - g + half * (2 * g - chips)) + parity, False)

        for p, first in SERVE:
            for i in range(1, tp):
                @pl.when(u == first + i - 1)
                def _():
                    serve(i, p)

        for p, at in REDUCE:
            @pl.when(u == at)
            def _():
                reduce(p)

        @pl.when(u == REDUCE[-1][1])
        def _():
            give()

    for h in range(heads):
        total = jnp.sum(running_sum[h], axis=1, keepdims=True)
        attended[:, h * head_dim : (h + 1) * head_dim] = (running_acc[h] / total).astype(BF16)

    def mix_to(j):
        return remote(
            parts.at[j], mix_theirs.at[j - 1], ms_sem.at[j - 1], mr_sem.at[j - 1], tp=lax.rem(t + j, tp)
        )

    for j in tuple(range(2, tp - 1)) + (1, tp - 1, 0):
        here = aligned(lax.rem(t + j, tp) * rows, rows)
        parts[j] = dot(attended[here, :], out_w[...]).astype(BF16)
        if j:
            mix_to(j).start()

    returned[:block, :] = back[:block, :]
    stages, batch = picks.shape[0], picks.shape[2]
    rweight = upright(rweight_ref)
    places = []
    for chosen_expert, rank in slot_columns(upright(routes_ref)):
        ahead = chosen_expert - e.astype(F32)
        ahead = jnp.where(ahead < 0, ahead + ep, ahead)
        place = jnp.where(ahead > ep // 2, 2 * (ep - ahead), jnp.maximum(2 * ahead - 1, 0))
        places.append(place * capacity + rank)
    for stage in range(stages):
        picks[stage] = jnp.concatenate(
            [chooser(place - stage * batch, batch) for place in places], axis=0
        ).astype(BF16)

    for j in range(1, tp):
        spread(j).wait_send()
        for p in range(pieces):
            back_to(j, p).wait_send()

        @pl.loop(0, groups)
        def _(g):
            forth(j, g).wait_send()

    @pl.loop(1, ep)
    def _(p):
        dispatch(p).wait_send()

    for half in range(2):
        share(0, half, 0).wait_send()

    @pl.loop(1, last + 1)
    def _(h):
        for way, half in WAYS:
            @pl.when(goes(way, half, h))
            def _():
                hop(way, half, h).wait_send()

            @pl.when(needed(way, half, h))
            def _():
                share(way, half, h).wait_send()

    total = parts[0].astype(F32)
    for j in range(1, tp):
        mix_to(j).wait_recv()
        total = total + mix_theirs[j - 1].astype(F32)
    mix_ref[...] = normalize(total, post_ref[...]).astype(BF16)
    for j in range(1, tp):
        mix_to(j).wait_send()

    for stage in range(stages):
        here = stage * batch

        @pl.loop(max(-(-here // capacity), 1), -(-(here + batch) // capacity))
        def _(p):
            give_back(p).wait()

        natural[pl.ds(here, batch), :] = from_wire(
            swap, returned[pl.ds(here * SUB, batch * SUB), :]
        )
        both = dot(picks[stage], natural[pl.ds(here, batch), :])
        result = rweight[:, :1] * both[:rows] + rweight[:, 1:2] * both[rows:]
        if stage:
            result = combined[...] + result
        if stage < stages - 1:
            combined[...] = result
        else:
            out_ref[...] = result.astype(BF16)


def hand_over(mix_ref, out_ref, mix_result, out_result):
    mix_result[...] = mix_ref[...]
    out_result[...] = out_ref[...]


def dma(*shape):
    return pltpu.SemaphoreType.DMA(shape)


def on_device(
    mixer_input, forget_cumsum, mixer_gain, query_weight, key_weight, value_weight, out_weight,
    post_gain, expert_input, expert_gain, routes, route_weight, expert_gate, expert_upward, expert_down,
):
    ep, tp = lax.axis_size("ep"), lax.axis_size("tp")
    rows, width = mixer_input.shape
    heads = forget_cumsum.shape[0]
    head_width = query_weight.shape[1]
    head_dim = head_width // heads
    span = rows * tp
    moe_rows, top = routes.shape
    experts = ep * expert_gate.shape[0]
    capacity = (moe_rows * top * 9 + 8 * experts - 1) // (8 * experts)
    slots = experts * capacity
    hidden = expert_gate.shape[2]
    vmem = pltpu.VMEM
    hops = ep // 4 + 3

    results = pl.pallas_call(
        functools.partial(kernel, capacity),
        name="block",
        out_shape=(
            jax.ShapeDtypeStruct((rows, width), BF16),
            jax.ShapeDtypeStruct((moe_rows, width), BF16),
        ),
        in_specs=[VM, VM, ANY, ANY, ANY, ANY, VM, VM, VM, VM, VM, VM, ANY, ANY, ANY],
        out_specs=(VM, VM),
        scratch_shapes=[
            vmem((span, width), BF16),
            vmem((3, width, head_width), BF16),
            vmem((span, head_width), BF16),
            vmem((ep, 2, span, head_width), BF16),
            vmem((head_width, width), BF16),
            vmem((heads, span, LANE), F32),
            vmem((heads, span, LANE), F32),
            vmem((heads, span, head_dim), F32),
            vmem((span, head_width), BF16),
            vmem((tp, rows, width), BF16),
            vmem((tp - 1, rows, width), BF16),
            vmem((slots, width), BF16),
            vmem((slots * SUB, LANE), BF16),
            vmem((tp, slots * SUB, LANE), BF16),
            vmem((1, width, hidden), BF16),
            vmem((1, width, hidden), BF16),
            vmem((1, hidden, width), BF16),
            vmem((tp, slots, width), BF16),
            vmem((tp - 1, slots, width), BF16),
            vmem((slots * SUB, LANE), BF16),
            vmem((slots * SUB, LANE), BF16),
            vmem((6, top * moe_rows, slots // 6), BF16),
            vmem((moe_rows, width), F32),
            dma(7), dma(tp - 1), dma(tp - 1), dma(ep), dma(ep), dma(tp - 1, 8), dma(tp - 1, 8),
            dma(tp - 1, 2), dma(tp - 1, 2), dma(ep), dma(ep), dma(tp - 1), dma(tp - 1),
            dma(2, 2, hops), dma(2, 2, hops), dma(2, 2, hops), dma(2, 2, hops),
        ],
        compiler_params=pltpu.CompilerParams(
            collective_id=0, has_side_effects=True, vmem_limit_bytes=63 * 1024 * 1024
        ),
    )(
        mixer_input, mixer_gain[None], query_weight, key_weight, value_weight, out_weight,
        post_gain[None], forget_cumsum, expert_input, expert_gain[None], routes.T, route_weight.T,
        expert_gate, expert_upward, expert_down,
    )
    return pl.pallas_call(
        hand_over,
        name="hand_over",
        out_shape=[jax.ShapeDtypeStruct(r.shape, r.dtype) for r in results],
        in_specs=[VM, VM],
        out_specs=[VM, VM],
    )(*results)


def solution(mesh):
    rows = P(("grp", "ep", "tp"), None)
    in_specs = (
        rows, P("tp", "grp"), P(), P(None, "tp"), P(None, "tp"), P(None, "tp"), P("tp", None), P(),
        rows, P(), rows, rows, P("ep", None, "tp"), P("ep", None, "tp"), P("ep", "tp", None),
    )
    return jax.shard_map(
        on_device, mesh=mesh, in_specs=in_specs, out_specs=(rows, rows), check_vma=False
    )
```
